256 devices in a mesh: ep: 16 (over y, x), tp: 16 (over z, core).
Axes of the slice: x: 4, y: 4, z: 8, core: 2. Of those that a mesh axis runs over, the one named last changes fastest.
Arguments:
- mix_tokens: bfloat16 [16384, 1, 1024], P(('ep', 'tp')), may hold values from -6 to 6
- mix_gain: float32 [1024], replicated, may hold values from 0.1 to 1.9
- w_query: bfloat16 [1024, 1024], replicated, may hold values from -0.1875 to 0.1875
- w_key: bfloat16 [1024, 256], replicated, may hold values from -0.1875 to 0.1875
- w_value: bfloat16 [1024, 256], replicated, may hold values from -0.1875 to 0.1875
- query_gain: float32 [64], replicated, may hold values from 1.2 to 14
- key_gain: float32 [64], replicated, may hold values from 1.2 to 14
- w_out: bfloat16 [1024, 1024], replicated, may hold values from -0.1875 to 0.1875
- expert_tokens: bfloat16 [32768, 1024], P(('ep', 'tp')), may hold values from -6 to 6
- expert_gain: float32 [1024], replicated, may hold values from 0.1 to 1.9
- route_ids: int32 [32768, 2], P(('ep', 'tp')), may hold values from 0 to 31, all different within a row; in each aligned block of 128 rows (0 to 127, 128 to 255, ...) at most 9 rows name the same one
- route_weights: float32 [32768, 2], P(('ep', 'tp')), may hold values from 0.1 to 1
- w_gate: bfloat16 [32, 1024, 4096], P('ep', None, 'tp'), may hold values from -0.1875 to 0.1875
- w_up: bfloat16 [32, 1024, 4096], P('ep', None, 'tp'), may hold values from -0.1875 to 0.1875
- w_down: bfloat16 [32, 4096, 1024], P('ep', 'tp'), may hold values from -0.09375 to 0.09375
Outputs:
- mix_out: bfloat16 [16384, 1, 1024], P(('ep', 'tp'))
- experts_out: bfloat16 [32768, 1024], P(('ep', 'tp'))
The draws below stay inside these ranges and needn't reach their ends.
Inputs may be any that keep to these rules, and one draw needn't show every extreme that they name: `route_ids`: each row names 2 different experts. Among the rows of one device no expert is named more than 9 times, and in every draw some expert is named exactly 9 times by the rows of some device.
All inputs are finite; a program needn't handle non-finite values.
Results may differ from the reference program's by a relative error of at most 0.018.
The reference program's roundings to bfloat16 on the way count: a program that leaves them out, or rounds other values in their place, can miss the bound.
Values may be sent and summed in bfloat16 or wider, within the bound.
A program may use at most 128 MiB of HBM per device.

```python
import math
import jax
import jax.numpy as jnp
import numpy as np
from jax import lax

D = 1024
HEADS = 16
KV_HEADS = 4
HEAD = 64
GRID_W = 64
FF = 4096
EXPERTS = 32
TOP_K = 2
SEQS = 1
LEN = 16384
TOK_EXP = 128
TOKENS = 32768
CAP = 9
N_TP = 16


def draw_gain_pair(base_key):
    base_gain = jax.random.uniform(jax.random.fold_in(base_key, 1), (HEAD,), jnp.float32, 1.2, 2.2)
    return base_gain


def draw_query_gain(key, part):
    return draw_gain_pair(jax.random.fold_in(key, 17))


def draw_key_gain(key, part):
    return draw_gain_pair(jax.random.fold_in(key, 29))


def shard_levels(own_key, dims, split, least, largest):
    loudness, own = 1.0, jax.random.fold_in(own_key, 6)
    for dim, shards_of in split:
        draws = jnp.exp(jax.random.uniform(jax.random.fold_in(own, dim), (shards_of,), jnp.float32, least / len(split), largest / len(split)))
        loudness = loudness * jnp.repeat(draws, dims[dim] // shards_of).reshape([-1 if axis == dim else 1 for axis in range(len(dims))])
    return loudness


def assign_block(own_key, own, number, rows, number_of, top, most, skew):
    sequence = jax.random.permutation(own_key, number_of)
    crowded, usual = load_shares(number_of, rows * top, most, skew, True), load_shares(number_of, rows * top, most, skew, False)
    places = jnp.arange(number_of)

    def named(sizes, offset_by):
        used = int((sizes > 0).sum())
        fixed = max(1, used // 4)
        shifted = fixed + (places - fixed + offset_by * (used - fixed)) % max(1, number_of - fixed)
        return jnp.zeros((number_of,), jnp.int32).at[sequence[jnp.where(places < fixed, places, shifted)]].set(jnp.asarray(sizes, jnp.int32))

    sizes = jnp.where(number % 4 == 0, named(crowded, number // 4), named(usual, number - number // 4 - 1))
    mixed = jax.random.permutation(jax.random.fold_in(own, 3), number_of)
    source_of, sink = mixed[0:number_of // 2 * 2:2], mixed[1:number_of // 2 * 2:2]
    room = jnp.minimum(sizes[source_of] - 1, most - sizes[sink]) // 2
    room = jnp.where((source_of == sequence[0]) | (sink == sequence[0]) | (sizes[sink] == 0), 0, jnp.maximum(room, 0))
    shifted = jax.random.randint(jax.random.fold_in(own, 4), (number_of // 2,), 0, 1 << 20) % (room + 1)
    sizes = sizes.at[source_of].add(-shifted).at[sink].add(shifted)
    members = jnp.searchsorted(jnp.cumsum(sizes), jnp.arange(rows * top), side="right").astype(jnp.int32)
    grid = members.reshape(top, rows).T
    grid = grid[jax.random.permutation(jax.random.fold_in(own, 1), rows)]
    offset_by = jax.random.randint(jax.random.fold_in(own, 2), (rows, 1), 0, top)
    return jnp.take_along_axis(grid, (jnp.arange(top)[None, :] + offset_by) % top, axis=1)


def load_shares(amount, total, most, skew, full):
    weights = [(1 << 20) // math.isqrt(standing ** skew) + 1 for standing in range(1, amount + 1)]
    largest = most if full else min(most, max(-(-total // amount), total * weights[0] // sum(weights)))
    least = 1 if total - largest >= amount - 1 else 0
    counts, spare = [largest] + [least] * (amount - 1), total - largest - least * (amount - 1)
    while spare > 0:
        free = [i for i in range(1, amount) if counts[i] < largest] or [i for i in range(1, amount) if counts[i] < most]
        mass, budget = sum([weights[i] for i in free]), spare
        for i in free:
            extra = min(most - counts[i], max(1, budget * weights[i] // mass), spare)
            counts[i] = counts[i] + extra
            spare = spare - extra
    return np.array(counts)


def centred(stream_key, extent, scale, limit, pieces=(), kind=jnp.bfloat16):
    factor_of = shard_levels(stream_key, extent, pieces, -0.22, 0.18) if pieces else 1.0
    values = jax.random.normal(stream_key, extent, jnp.float32) * scale * factor_of
    return jnp.minimum(jnp.maximum(values, -limit), limit).astype(kind)


def setup_inputs(seed: int = 0) -> dict:
    key_list = jax.random.split(jax.random.key(seed), 16)
    mix_tokens = centred(key_list[0], (LEN, SEQS, D), 1.0, 6.0, ((0, 256),))
    mix_gain = jnp.clip(1.0 + 0.18 * jax.random.normal(key_list[1], (D,), jnp.float32), 0.1, 1.9)
    w_query = centred(key_list[2], (D, HEADS * HEAD), D ** -0.5, 0.1875)
    w_key = centred(key_list[3], (D, KV_HEADS * HEAD), D ** -0.5, 0.1875)
    w_value = centred(key_list[4], (D, KV_HEADS * HEAD), D ** -0.5, 0.1875)
    query_gain = draw_query_gain(jax.random.fold_in(key_list[15], 71), 0)
    key_gain = draw_key_gain(jax.random.fold_in(key_list[15], 71), 0)
    w_out = centred(key_list[7], (HEADS * HEAD, D), (HEADS * HEAD) ** -0.5, 0.1875)
    expert_tokens = centred(key_list[8], (TOKENS, D), 1.0, 6.0, ((0, 256),))
    expert_gain = jnp.clip(1.0 + 0.18 * jax.random.normal(key_list[9], (D,), jnp.float32), 0.1, 1.9)
    route_ids_keys = jax.random.split(jax.random.fold_in(key_list[10], 1), TOKENS // TOK_EXP)
    route_ids_turns = jax.random.permutation(jax.random.fold_in(key_list[10], 3), TOKENS // TOK_EXP)
    route_ids = jax.vmap(lambda own, number: assign_block(jax.random.fold_in(key_list[10], 2), own, number, TOK_EXP, EXPERTS, TOP_K, CAP, 1))(route_ids_keys, route_ids_turns).reshape((TOKENS, TOP_K))
    route_weights = jnp.clip(jnp.exp(math.log(1.0) - 2.3025851 * jax.random.uniform(key_list[11], (TOKENS, TOP_K), jnp.float32) ** shard_levels(key_list[11], (TOKENS, TOP_K), ((0, 256),), -0.2, 0.2)), 0.1, 1.0)
    w_gate = centred(key_list[12], (EXPERTS, D, FF), D ** -0.5, 0.1875, ((0, 16), (2, 16)))
    w_up = centred(key_list[13], (EXPERTS, D, FF), D ** -0.5, 0.1875, ((0, 16), (2, 16)))
    w_down = centred(key_list[14], (EXPERTS, FF, D), FF ** -0.5, 0.09375, ((0, 16), (1, 16)))
    return dict(mix_tokens=mix_tokens, mix_gain=mix_gain, w_query=w_query, w_key=w_key, w_value=w_value, query_gain=query_gain, key_gain=key_gain, w_out=w_out, expert_tokens=expert_tokens, expert_gain=expert_gain, route_ids=route_ids, route_weights=route_weights, w_gate=w_gate, w_up=w_up, w_down=w_down)


epsilon = 1e-06

def normalize(values, gain_vec):
    widened = values.astype(jnp.float32)
    return widened * lax.rsqrt(lax.optimization_barrier(jnp.mean(widened * widened, axis=-1, keepdims=True)) + epsilon) * gain_vec

def angle_tables(positions, head_size):
    quarter = head_size // 4
    frequency = 10000.0 ** (-jnp.arange(quarter, dtype=jnp.float32) / quarter)
    grid_pos = jnp.stack([positions // GRID_W, positions % GRID_W], axis=-1).astype(jnp.float32)
    angles = grid_pos[:, :, None] * frequency[None, None, :]
    return (jnp.cos(angles), jnp.sin(angles))

def turn(values, cosine_table, sine_table):
    shaped = values.shape
    quarter = shaped[-1] // 4
    leading = (shaped[0],) + (1,) * (len(shaped) - 2) + (2, quarter)
    cosine_table = cosine_table.reshape(leading)
    sine_table = sine_table.reshape(leading)
    halves = values.reshape(shaped[:-1] + (2, 2, quarter))
    first_part = halves[..., 0, :]
    second_part = halves[..., 1, :]
    turned = jnp.stack([first_part * cosine_table - second_part * sine_table, first_part * sine_table + second_part * cosine_table], axis=-2)
    return turned.reshape(shaped)

def mixer_reference(mix_tokens, mix_gain, w_query, w_key, w_value, query_gain, key_gain, w_out):
    normed = normalize(mix_tokens, mix_gain).astype(jnp.bfloat16)
    queries = jnp.dot(normed, w_query, preferred_element_type=jnp.float32).astype(jnp.bfloat16)
    keys_raw = jnp.dot(normed, w_key, preferred_element_type=jnp.float32).astype(jnp.bfloat16)
    values = jnp.dot(normed, w_value, preferred_element_type=jnp.float32).astype(jnp.bfloat16)
    group_size = HEADS // KV_HEADS
    cosine_table, sine_table = angle_tables(jnp.arange(LEN, dtype=jnp.int32), HEAD)
    query_heads = normalize(queries.reshape(LEN, SEQS, HEADS, HEAD), query_gain)
    turned_queries = turn(query_heads, cosine_table, sine_table).astype(jnp.bfloat16)
    turned_queries = turned_queries.reshape(LEN, SEQS, KV_HEADS, group_size, HEAD)
    key_heads = normalize(keys_raw.reshape(LEN, SEQS, KV_HEADS, HEAD), key_gain)
    turned_keys = turn(key_heads, cosine_table, sine_table).astype(jnp.bfloat16).astype(jnp.float32)
    value_heads = values.reshape(LEN, SEQS, KV_HEADS, HEAD).astype(jnp.float32)
    block_rows = math.gcd(LEN, 128)

    def attend(query_block):
        scores = jnp.einsum('qskgd,lskd->qskgl', query_block.astype(jnp.float32), turned_keys) * HEAD ** (-0.5)
        row_max = lax.optimization_barrier(jnp.max(scores, axis=-1, keepdims=True))
        raised = jnp.exp(scores - row_max)
        totals = lax.optimization_barrier(jnp.sum(raised, axis=-1))
        weights = lax.optimization_barrier(raised.astype(jnp.bfloat16)).astype(jnp.float32)
        mixed = jnp.einsum('qskgl,lskd->qskgd', weights, value_heads) / totals[..., None]
        return mixed.astype(jnp.bfloat16)
    blocks = turned_queries.reshape(LEN // block_rows, block_rows, SEQS, KV_HEADS, group_size, HEAD)
    outputs = lax.map(attend, blocks)
    mixed_heads = outputs.reshape(LEN, SEQS, HEADS * HEAD)
    return jnp.dot(mixed_heads, w_out, preferred_element_type=jnp.float32).astype(jnp.bfloat16)

def experts_reference(expert_tokens, expert_gain, route_ids, route_weights, w_gate, w_up, w_down):
    tok_total = expert_tokens.shape[0]
    block_count = tok_total // TOK_EXP
    normed = normalize(expert_tokens, expert_gain).astype(jnp.bfloat16)
    grouped = route_ids.reshape(block_count, TOK_EXP * TOP_K)
    matches = (grouped[:, :, None] == jnp.arange(EXPERTS, dtype=jnp.int32)[None, None, :]).astype(jnp.int32)
    rank_ids = lax.optimization_barrier(jnp.sum((jnp.cumsum(matches, axis=1) - 1) * matches, axis=2)).astype(jnp.int32)
    slot_ids = (jnp.arange(block_count, dtype=jnp.int32)[:, None] * CAP + rank_ids).reshape(-1).astype(jnp.int32)
    flat_ids = grouped.reshape(-1).astype(jnp.int32)
    token_ids = (jnp.arange(tok_total * TOP_K, dtype=jnp.int32) // TOP_K).astype(jnp.int32)
    buffer_rows = jnp.zeros((EXPERTS, block_count * CAP, D), jnp.bfloat16).at[flat_ids, slot_ids].set(normed[token_ids])

    def run_expert(operands):
        rows_in, gate_w, up_w, down_w = operands
        gate_act = jnp.dot(rows_in, gate_w, preferred_element_type=jnp.float32)
        up_act = jnp.dot(rows_in, up_w, preferred_element_type=jnp.float32)
        hidden = (jax.nn.silu(gate_act) * up_act).astype(jnp.bfloat16)
        hidden_groups = hidden.reshape(-1, N_TP, FF // N_TP).astype(jnp.float32)
        down_groups = down_w.reshape(N_TP, FF // N_TP, D).astype(jnp.float32)
        group_sums = jnp.einsum('ngf,gfd->ngd', hidden_groups, down_groups).astype(jnp.bfloat16)
        group_sums = lax.optimization_barrier(group_sums).astype(jnp.float32)
        return lax.optimization_barrier(jnp.sum(group_sums, axis=1)).astype(jnp.bfloat16)
    outputs = lax.map(run_expert, (buffer_rows, w_gate, w_up, w_down))
    picked = outputs[flat_ids, slot_ids].reshape(tok_total, TOP_K, D)
    combined = lax.optimization_barrier(jnp.sum(route_weights[:, :, None] * picked.astype(jnp.float32), axis=1))
    return combined.astype(jnp.bfloat16)

def reference(mix_tokens, mix_gain, w_query, w_key, w_value, query_gain, key_gain, w_out, expert_tokens, expert_gain, route_ids, route_weights, w_gate, w_up, w_down):
    mix_out = mixer_reference(mix_tokens, mix_gain, w_query, w_key, w_value, query_gain, key_gain, w_out)
    experts_out = experts_reference(expert_tokens, expert_gain, route_ids, route_weights, w_gate, w_up, w_down)
    return (mix_out, experts_out)
```

```python
import functools
import math

import jax
import jax.numpy as jnp
from jax import lax
from jax.experimental import pallas as pl
from jax.experimental.pallas import tpu as pltpu
from jax.sharding import PartitionSpec as P

HEAD = 64
GRID_W = 64
EXP2_SCALE = HEAD ** (-0.5) * math.log2(math.e)
MESH = pl.DeviceIdType.MESH
MIB = 1024 * 1024


epsilon = 1e-06


def normalize(values, gain_vec):
    widened = values.astype(jnp.float32)
    return (
        widened
        * lax.rsqrt(jnp.mean(widened * widened, axis=-1, keepdims=True) + epsilon)
        * gain_vec
    )


def angle_tables(positions, head_size):
    quarter = head_size // 4
    frequency = 10000.0 ** (-jnp.arange(quarter, dtype=jnp.float32) / quarter)
    grid_pos = jnp.stack([positions // GRID_W, positions % GRID_W], axis=-1).astype(jnp.float32)
    angles = grid_pos[:, :, None] * frequency[None, None, :]
    return (jnp.cos(angles), jnp.sin(angles))


def turn(values, cosine_table, sine_table):
    shaped = values.shape
    quarter = shaped[-1] // 4
    leading = (shaped[0],) + (1,) * (len(shaped) - 2) + (2, quarter)
    cosine_table = cosine_table.reshape(leading)
    sine_table = sine_table.reshape(leading)
    halves = values.reshape(shaped[:-1] + (2, 2, quarter))
    first_part = halves[..., 0, :]
    second_part = halves[..., 1, :]
    turned = jnp.stack(
        [
            first_part * cosine_table - second_part * sine_table,
            first_part * sine_table + second_part * cosine_table,
        ],
        axis=-2,
    )
    return turned.reshape(shaped)


def meet(peers):
    barrier = pltpu.get_barrier_semaphore()
    for peer in peers:
        pl.semaphore_signal(barrier, inc=1, device_id=peer, device_id_type=MESH)
    pl.semaphore_wait(barrier, len(peers))


def exchange_body(x_ref, y_ref, x_out, y_out, x_send, x_recv, y_send, y_recv):
    lanes = []
    for axis, source, target, send, recv in (
        ("tp", y_ref, y_out, y_send, y_recv),
        ("ep", x_ref, x_out, x_send, x_recv),
    ):
        lanes.append((axis, lax.axis_index(axis), source.shape[0], source, target, send, recv))
    meet([{axis: lax.rem(me + d, n)} for axis, me, n, *_ in lanes for d in range(1, n)])
    copies = []
    for axis, me, n, source, target, send, recv in lanes:
        for d in range(1, n):
            peer = lax.rem(me + d, n)
            copy = pltpu.make_async_remote_copy(
                src_ref=source.at[peer],
                dst_ref=target.at[me],
                send_sem=send.at[d],
                recv_sem=recv.at[d],
                device_id={axis: peer},
                device_id_type=MESH,
            )
            copy.start()
            copies.append(copy)
    for axis, me, n, source, target, send, recv in lanes:
        target[me] = source[me]
    for copy in copies:
        copy.wait()


def exchange(x, y, collective_id):
    vmem = pl.BlockSpec(memory_space=pltpu.VMEM)
    x_count, y_count = x.shape[0], y.shape[0]
    return pl.pallas_call(
        exchange_body,
        out_shape=[jax.ShapeDtypeStruct(a.shape, a.dtype) for a in (x, y)],
        in_specs=[vmem, vmem],
        out_specs=[vmem, vmem],
        scratch_shapes=[
            pltpu.SemaphoreType.DMA((x_count,)),
            pltpu.SemaphoreType.DMA((x_count,)),
            pltpu.SemaphoreType.DMA((y_count,)),
            pltpu.SemaphoreType.DMA((y_count,)),
        ],
        name="exchange",
        cost_estimate=pl.CostEstimate(flops=10**10, bytes_accessed=10**6, transcendentals=0),
        compiler_params=pltpu.CompilerParams(
            collective_id=collective_id, has_side_effects=True, vmem_limit_bytes=24 * MIB
        ),
    )(x, y)


def ring_places():
    me = lax.axis_index("tp")
    chips = lax.axis_size("tp") // 2
    chip, core = me // 2, lax.rem(me, 2)
    ahead = lax.rem(chip + 1 - 2 * core + chips, chips) * 2 + core
    behind = lax.rem(chip - 1 + 2 * core + chips, chips) * 2 + core
    partner = chip * 2 + 1 - core
    return {"tp": ahead}, {"tp": behind}, {"tp": partner}


def gather_body(
    rows_ref,
    gate_ref,
    up_ref,
    down_ref,
    own_out,
    pair_out,
    held,
    own_part,
    pair_part,
    load_sem,
    ring_send,
    ring_recv,
    pair_send,
    pair_recv,
    own_sem,
    part_send,
    part_recv,
):
    pieces, _, piece_rows, width = held.shape
    ahead, behind, partner = ring_places()
    loads = [
        pltpu.make_async_copy(rows_ref.at[j], held.at[j, 0], load_sem.at[j]) for j in range(2)
    ]
    for load in loads:
        load.start()

    def ring_copy(i):
        return pltpu.make_async_remote_copy(
            src_ref=held.at[i, 0],
            dst_ref=held.at[i + 2, 0],
            send_sem=ring_send.at[i],
            recv_sem=ring_recv.at[i + 2],
            device_id=ahead,
            device_id_type=MESH,
        )

    def ring_arrival(i):
        return pltpu.make_async_remote_copy(
            src_ref=held.at[i, 0],
            dst_ref=held.at[i, 0],
            send_sem=ring_send.at[i],
            recv_sem=ring_recv.at[i],
            device_id=ahead,
            device_id_type=MESH,
        )

    def pair_copy(i):
        return pltpu.make_async_remote_copy(
            src_ref=held.at[i, 0],
            dst_ref=held.at[i, 1],
            send_sem=pair_send.at[i],
            recv_sem=pair_recv.at[i],
            device_id=partner,
            device_id_type=MESH,
        )

    def part_copy(i):
        return pltpu.make_async_remote_copy(
            src_ref=pair_part.at[i],
            dst_ref=pair_out.at[i],
            send_sem=part_send.at[i],
            recv_sem=part_recv.at[i],
            device_id=partner,
            device_id_type=MESH,
        )

    def own_copy(i):
        return pltpu.make_async_copy(own_part.at[i], own_out.at[i], own_sem.at[i])

    meet([ahead, behind, partner])
    for load in loads:
        load.wait()

    def step(i, _):
        @pl.when(i < pieces)
        def _():
            @pl.when(i >= 2)
            def _():
                ring_arrival(i).wait_recv()

            @pl.when(i < pieces - 2)
            def _():
                ring_copy(i).start()

            pair_copy(i).start()

        @pl.when(jnp.logical_and(i >= 1, i <= pieces))
        def _():
            piece = i - 1
            expert = lax.rem(piece, 2)
            pair_copy(piece).wait_recv()
            rows = held[piece].reshape(2 * piece_rows, width)
            gate_act = jnp.dot(rows, gate_ref[expert], preferred_element_type=jnp.float32)
            up_act = jnp.dot(rows, up_ref[expert], preferred_element_type=jnp.float32)
            hidden = (gate_act / (1.0 + jnp.exp(-gate_act)) * up_act).astype(jnp.bfloat16)
            sums = jnp.dot(hidden, down_ref[expert], preferred_element_type=jnp.float32)
            sums = sums.astype(jnp.bfloat16)
            own_part[piece] = sums[:piece_rows]
            pair_part[piece] = sums[piece_rows:]

        @pl.when(i >= 2)
        def _():
            own_copy(i - 2).start()
            part_copy(i - 2).start()

        return 0

    lax.fori_loop(0, pieces + 2, step, 0)

    def finish(i, _):
        @pl.when(i < pieces - 2)
        def _():
            ring_copy(i).wait_send()

        pair_copy(i).wait_send()
        own_copy(i).wait()
        part_copy(i).wait()
        return 0

    lax.fori_loop(0, pieces, finish, 0)


def gather_experts(rows, w_gate, w_up, w_down):
    pieces = lax.axis_size("tp")
    _, piece_rows, width = rows.shape
    vmem, hbm = pl.BlockSpec(memory_space=pltpu.VMEM), pl.BlockSpec(memory_space=pl.ANY)
    part = jax.ShapeDtypeStruct((pieces, piece_rows, width), jnp.bfloat16)
    dma = pltpu.SemaphoreType.DMA
    return pl.pallas_call(
        gather_body,
        out_shape=[part, part],
        in_specs=[hbm, vmem, vmem, vmem],
        out_specs=[hbm, hbm],
        scratch_shapes=[
            pltpu.VMEM((pieces, 2, piece_rows, width), jnp.bfloat16),
            pltpu.VMEM((pieces, piece_rows, width), jnp.bfloat16),
            pltpu.VMEM((pieces, piece_rows, width), jnp.bfloat16),
            dma((2,)),
        ]
        + [dma((pieces,)) for _ in range(7)],
        name="gather_experts",
        cost_estimate=pl.CostEstimate(
            flops=5 * 10**10, bytes_accessed=2 * 10**7, transcendentals=0
        ),
        compiler_params=pltpu.CompilerParams(
            collective_id=1, has_side_effects=True, vmem_limit_bytes=44 * MIB
        ),
    )(rows, w_gate, w_up, w_down)


def scatter_body(
    query_tile,
    key_block,
    query_ref,
    pair_ref,
    own_hbm,
    part_hbm,
    sums_out,
    mixed_out,
    own_part,
    pair_part,
    arrived,
    leaving,
    row_max,
    row_sum,
    row_acc,
    own_sem,
    part_sem,
    ring_send,
    ring_recv,
):
    pieces = own_part.shape[0]
    tiles, blocks = query_ref.shape[0] // query_tile, pair_ref.shape[0] // key_block
    slices = tiles * blocks // pieces
    ahead, behind, _ = ring_places()

    def loads(i):
        slot = lax.rem(i + 2, pieces)
        return (
            pltpu.make_async_copy(own_hbm.at[slot], own_part.at[i], own_sem.at[i]),
            pltpu.make_async_copy(part_hbm.at[slot], pair_part.at[i], part_sem.at[i]),
        )

    def ring_copy(i):
        return pltpu.make_async_remote_copy(
            src_ref=leaving.at[i],
            dst_ref=arrived.at[i],
            send_sem=ring_send.at[i],
            recv_sem=ring_recv.at[i],
            device_id=ahead,
            device_id_type=MESH,
        )

    def start_loads(i, _):
        for load in loads(i):
            load.start()
        return 0

    lax.fori_loop(0, pieces, start_loads, 0)
    meet([ahead, behind])
    row_max[...] = jnp.full(row_max.shape, -1e30, jnp.float32)
    row_sum[...] = jnp.zeros(row_sum.shape, jnp.float32)
    row_acc[...] = jnp.zeros(row_acc.shape, jnp.float32)

    def attend_slice(number):
        block, tile = number // tiles, lax.rem(number, tiles)
        first = pl.multiple_of(tile * query_tile, query_tile)
        queries = query_ref[pl.ds(first, query_tile), :]
        pairs = pair_ref[pl.ds(pl.multiple_of(block * key_block, key_block), key_block), :]
        scores = lax.dot_general(
            queries, pairs, (((1,), (1,)), ((), ())), preferred_element_type=jnp.float32
        )
        old_max = row_max[tile][:, :1]
        new_max = jnp.maximum(old_max, jnp.max(scores, axis=1, keepdims=True))
        shrink = jnp.exp2((old_max - new_max) * EXP2_SCALE)
        raised = jnp.exp2((scores - new_max) * EXP2_SCALE)
        lane_sums = raised[:, :128]
        for lane in range(128, key_block, 128):
            lane_sums = lane_sums + raised[:, lane : lane + 128]
        row_max[tile] = jnp.broadcast_to(new_max, (query_tile, 128))
        row_sum[tile] = row_sum[tile] * shrink + lane_sums
        row_acc[tile] = row_acc[tile] * shrink + jnp.dot(
            raised.astype(jnp.bfloat16), pairs, preferred_element_type=jnp.float32
        )

    def step(i, _):
        for load in loads(i):
            load.wait()

        @pl.when(i < 2)
        def _():
            total = own_part[i].astype(jnp.float32) + pair_part[i].astype(jnp.float32)
            leaving[i] = total.astype(jnp.bfloat16)

        @pl.when(i >= 2)
        def _():
            ring_copy(i - 2).wait_recv()
            total = own_part[i].astype(jnp.float32) + pair_part[i].astype(jnp.float32)
            total = (total + arrived[i - 2].astype(jnp.float32)).astype(jnp.bfloat16)

            @pl.when(i < pieces - 2)
            def _():
                leaving[i] = total

            @pl.when(i >= pieces - 2)
            def _():
                sums_out[i - (pieces - 2)] = total

        @pl.when(i < pieces - 2)
        def _():
            ring_copy(i).start()

        for part in range(slices):
            attend_slice(i * slices + part)
        return 0

    lax.fori_loop(0, pieces, step, 0)

    def finish(i, _):
        ring_copy(i).wait_send()
        return 0

    lax.fori_loop(0, pieces - 2, finish, 0)
    for tile in range(tiles):
        mixed = row_acc[tile] / jnp.sum(row_sum[tile], axis=1, keepdims=True)
        mixed_out[tile * query_tile : (tile + 1) * query_tile, :] = mixed.astype(jnp.bfloat16)


def scatter_experts(queries, pairs, own_part, pair_part):
    pieces, piece_rows, width = own_part.shape
    rows, keys = queries.shape[0], pairs.shape[0]
    query_tile, key_block = math.gcd(rows, 256), math.gcd(keys, 2048)
    tiles = rows // query_tile
    vmem, hbm = pl.BlockSpec(memory_space=pltpu.VMEM), pl.BlockSpec(memory_space=pl.ANY)
    dma = pltpu.SemaphoreType.DMA
    piece = (piece_rows, width)
    return pl.pallas_call(
        functools.partial(scatter_body, query_tile, key_block),
        out_shape=[
            jax.ShapeDtypeStruct((2,) + piece, jnp.bfloat16),
            jax.ShapeDtypeStruct((rows, 2 * HEAD), jnp.bfloat16),
        ],
        in_specs=[vmem, vmem, hbm, hbm],
        out_specs=[vmem, vmem],
        scratch_shapes=[
            pltpu.VMEM((pieces,) + piece, jnp.bfloat16),
            pltpu.VMEM((pieces,) + piece, jnp.bfloat16),
            pltpu.VMEM((pieces - 2,) + piece, jnp.bfloat16),
            pltpu.VMEM((pieces - 2,) + piece, jnp.bfloat16),
            pltpu.VMEM((tiles, query_tile, 128), jnp.float32),
            pltpu.VMEM((tiles, query_tile, 128), jnp.float32),
            pltpu.VMEM((tiles, query_tile, 128), jnp.float32),
            dma((pieces,)),
            dma((pieces,)),
            dma((pieces,)),
            dma((pieces,)),
        ],
        name="scatter_experts",
        cost_estimate=pl.CostEstimate(
            flops=5 * 10**10, bytes_accessed=2 * 10**7, transcendentals=0
        ),
        compiler_params=pltpu.CompilerParams(
            collective_id=2, has_side_effects=True, vmem_limit_bytes=52 * MIB
        ),
    )(queries, pairs, own_part, pair_part)


def body(
    mix_tokens,
    mix_gain,
    w_query,
    w_key,
    w_value,
    query_gain,
    key_gain,
    w_out,
    expert_tokens,
    expert_gain,
    route_ids,
    route_weights,
    w_gate,
    w_up,
    w_down,
):
    tp_count, ep_count = lax.axis_size("tp"), lax.axis_size("ep")
    seq_rows, sequences, model_width = mix_tokens.shape
    key_heads = w_key.shape[1] // HEAD
    half_rows = seq_rows // 2
    mix_normed = normalize(mix_tokens[:, 0, :], mix_gain).astype(jnp.bfloat16)
    queries = jnp.dot(mix_normed, w_query, preferred_element_type=jnp.float32).astype(jnp.bfloat16)
    keys_raw = jnp.dot(mix_normed, w_key, preferred_element_type=jnp.float32).astype(jnp.bfloat16)
    values = jnp.dot(mix_normed, w_value, preferred_element_type=jnp.float32).astype(jnp.bfloat16)
    by_head = queries.reshape(2, half_rows, tp_count, HEAD)
    by_head = jnp.transpose(by_head, (2, 1, 0, 3)).reshape(tp_count, half_rows, 2 * HEAD)
    key_value = jnp.concatenate(
        [keys_raw.reshape(seq_rows, key_heads, HEAD), values.reshape(seq_rows, key_heads, HEAD)],
        axis=-1,
    )
    key_value = jnp.repeat(jnp.transpose(key_value, (1, 0, 2)), tp_count // key_heads, axis=0)
    packed = jnp.concatenate([key_value, by_head], axis=1)

    tok_count = expert_tokens.shape[0]
    top_count = route_ids.shape[1]
    local_experts = w_gate.shape[0]
    expert_count = local_experts * ep_count
    capacity = tok_count * top_count * 9 // (8 * expert_count)
    slot_count = ep_count * capacity * local_experts
    normed = normalize(expert_tokens, expert_gain).astype(jnp.bfloat16)
    flat_ids = route_ids.reshape(-1)
    matches = (flat_ids[:, None] == jnp.arange(expert_count, dtype=jnp.int32)[None, :]).astype(
        jnp.int32
    )
    rank_ids = jnp.sum((jnp.cumsum(matches, axis=0) - 1) * matches, axis=1)
    slot_ids = (
        flat_ids // local_experts * local_experts + flat_ids % local_experts
    ) * capacity + rank_ids
    chosen = slot_ids.reshape(tok_count, top_count)
    slots = jnp.arange(slot_count, dtype=jnp.int32)
    hits = chosen[:, :, None] == slots[None, None, :]
    dispatch = jnp.sum(hits.astype(jnp.bfloat16), axis=1)
    outgoing = lax.dot_general(
        dispatch, normed, (((0,), (0,)), ((), ())), preferred_element_type=jnp.float32
    ).astype(jnp.bfloat16)
    lane_rows = local_experts * capacity * model_width // 128
    outgoing = outgoing.reshape(ep_count, lane_rows, 128)

    incoming, arrived = exchange(outgoing, packed, 0)

    span_rows = tp_count * seq_rows
    positions = lax.axis_index("ep") * span_rows + jnp.arange(span_rows, dtype=jnp.int32)
    cosine_table, sine_table = angle_tables(positions, HEAD)
    pair_rows = arrived[:, :seq_rows, :].reshape(span_rows, 2 * HEAD)
    own_queries = arrived[:, seq_rows:, :].reshape(tp_count, half_rows, 2, HEAD)
    own_queries = jnp.transpose(own_queries, (0, 2, 1, 3)).reshape(span_rows, HEAD)
    own_queries = turn(normalize(own_queries, query_gain), cosine_table, sine_table)
    padded_queries = jnp.pad(own_queries.astype(jnp.bfloat16), ((0, 0), (0, HEAD)))
    own_keys = turn(normalize(pair_rows[:, :HEAD], key_gain), cosine_table, sine_table)
    key_pairs = jnp.concatenate([own_keys.astype(jnp.bfloat16), pair_rows[:, HEAD:]], axis=-1)
    pairs = lax.all_gather(key_pairs, "ep", axis=0, tiled=True)

    own_rows = ep_count * capacity
    rows = incoming.reshape(ep_count, local_experts, capacity, model_width)
    rows = jnp.transpose(rows, (1, 0, 2, 3)).reshape(local_experts, own_rows, model_width)
    own_part, pair_part = gather_experts(rows, w_gate, w_up, w_down)
    summed, mixed = scatter_experts(padded_queries, pairs, own_part, pair_part)

    summed = summed.reshape(local_experts, ep_count, capacity, model_width)
    summed = jnp.transpose(summed, (1, 0, 2, 3)).reshape(ep_count, lane_rows, 128)
    results, heads = exchange(summed, mixed.reshape(tp_count, seq_rows, 2 * HEAD), 3)

    heads = jnp.transpose(heads[:, :, HEAD:], (1, 0, 2)).reshape(seq_rows, tp_count * HEAD)
    mix_out = jnp.dot(heads, w_out, preferred_element_type=jnp.float32).astype(jnp.bfloat16)
    results = results.reshape(slot_count, model_width)
    picked = jnp.take(results, slot_ids, axis=0).reshape(tok_count, top_count, model_width)
    combined = jnp.sum(route_weights[:, :, None] * picked.astype(jnp.float32), axis=1)
    return (mix_out[:, None, :], combined.astype(jnp.bfloat16))


def solution(mesh):
    placed = (
        P(("ep", "tp"), None, None),
        P(),
        P(),
        P(),
        P(),
        P(),
        P(),
        P(),
        P(("ep", "tp"), None),
        P(),
        P(("ep", "tp"), None),
        P(("ep", "tp"), None),
        P("ep", None, "tp"),
        P("ep", None, "tp"),
        P("ep", "tp", None),
    )
    return jax.shard_map(
        body,
        mesh=mesh,
        in_specs=placed,
        out_specs=(P(("ep", "tp"), None, None), P(("ep", "tp"), None)),
        check_vma=False,
    )
```

```python
import functools
import math

import jax
import jax.numpy as jnp
from jax import lax
from jax.experimental import pallas as pl
from jax.experimental.pallas import tpu as pltpu
from jax.sharding import PartitionSpec as P

HEAD = 64
GRID_W = 64
LANES = 128
EXP2_SCALE = HEAD ** (-0.5) * math.log2(math.e)
MESH = pl.DeviceIdType.MESH
MIB = 1024 * 1024
BF16, F32 = jnp.bfloat16, jnp.float32
VMEM_SPEC = pl.BlockSpec(memory_space=pltpu.VMEM)
HBM_SPEC = pl.BlockSpec(memory_space=pltpu.HBM)
DMA = pltpu.SemaphoreType.DMA


epsilon = 1e-06


def normalize(values, gain_vec):
    widened = values.astype(F32)
    return (
        widened
        * lax.rsqrt(jnp.mean(widened * widened, axis=-1, keepdims=True) + epsilon)
        * gain_vec
    )


def matmul(left, right):
    return jnp.dot(left, right, preferred_element_type=F32)


def angle_tables(positions, head_size):
    quarter = head_size // 4
    frequency = 10000.0 ** (-jnp.arange(quarter, dtype=F32) / quarter)
    grid_pos = jnp.stack([positions // GRID_W, positions % GRID_W], axis=-1).astype(F32)
    angles = grid_pos[:, :, None] * frequency[None, None, :]
    return (jnp.cos(angles), jnp.sin(angles))


def lane_tables(positions):
    cosine, sine = angle_tables(positions, HEAD)
    rows = cosine.shape[0]
    cosine = jnp.stack([cosine, cosine], axis=2).reshape(rows, HEAD)
    sine = jnp.stack([-sine, sine], axis=2).reshape(rows, HEAD)
    return jnp.tile(cosine, (1, LANES // HEAD)), jnp.tile(sine, (1, LANES // HEAD))


def greet(peers):
    barrier = pltpu.get_barrier_semaphore()
    for peer in peers:
        pl.semaphore_signal(barrier, inc=1, device_id=peer, device_id_type=MESH)


def await_greetings(count):
    pl.semaphore_wait(pltpu.get_barrier_semaphore(), count)


def axis_peers(axis):
    me, count = lax.axis_index(axis), lax.axis_size(axis)
    return [lax.rem(me + d, count) for d in range(count)]


def remote(source, target, send_sem, recv_sem, device_id):
    return pltpu.make_async_remote_copy(
        src_ref=source,
        dst_ref=target,
        send_sem=send_sem,
        recv_sem=recv_sem,
        device_id=device_id,
        device_id_type=MESH,
    )


def exchange_copies(axis, sources, targets, sends, recvs):
    me = lax.axis_index(axis)
    return [
        remote(source(peer), target(me), send.at[d], recv.at[d], {axis: peer})
        for d, peer in enumerate(axis_peers(axis))
        if d > 0
        for source, target, send, recv in zip(sources, targets, sends, recvs)
    ]


def iota(shape, axis):
    return lax.broadcasted_iota(jnp.int32, shape, axis)


def slot_rows(id_rows, experts, capacity):
    choices, tokens = id_rows.shape
    marks = [
        (iota((experts, tokens), 0) == id_rows[k : k + 1, :]).astype(F32) for k in range(choices)
    ]
    earlier = (iota((tokens, tokens), 0) < iota((tokens, tokens), 1)).astype(BF16)
    ranks = matmul(functools.reduce(jnp.add, marks).astype(BF16), earlier)
    main, last = [], []
    for k in range(choices):
        rank = jnp.sum(marks[k] * ranks, axis=0, keepdims=True).astype(jnp.int32)
        ids = id_rows[k : k + 1, :]
        main.append(jnp.where(rank < capacity - 1, ids * (capacity - 1) + rank, -1))
        last.append(jnp.where(rank == capacity - 1, ids, -1))
    return main, last


def pick(rows, columns, first, stride):
    wanted = iota((rows, columns), 0) * stride + first
    return (iota((rows, columns), 1) == wanted).astype(BF16)


def place(rows, columns, first, stride):
    wanted = iota((rows, columns), 1) * stride + first
    return (iota((rows, columns), 0) == wanted).astype(BF16)


def head_turner(cosine, sine, pair_sums):
    lane = iota(cosine.shape, 1)
    quarter = HEAD // 4

    def turned(raw, gain):
        values = raw.astype(BF16).astype(F32)
        squares = values * values
        high = squares.astype(BF16)
        low = (squares - high.astype(F32)).astype(BF16)
        sums = matmul(high, pair_sums) + matmul(low, pair_sums)
        values = values * lax.rsqrt(sums * (1.0 / HEAD) + epsilon) * gain
        partner = jnp.where(
            lax.rem(lane, 2 * quarter) < quarter,
            pltpu.roll(values, LANES - quarter, 1),
            pltpu.roll(values, quarter, 1),
        )
        return (values * cosine + partner * sine).astype(BF16).astype(F32)

    return turned


def dispatch_body(
    mix_ref,
    mix_gain_ref,
    query_hbm,
    key_hbm,
    value_hbm,
    query_gain_ref,
    key_gain_ref,
    cosine_ref,
    sine_ref,
    token_ref,
    token_gain_ref,
    ids_ref,
    head_out,
    main_out,
    last_out,
    w_query,
    w_key,
    w_value,
    head_send,
    main_send,
    last_send,
    last_recv,
    load_sem,
    head_sems,
    main_sems,
    last_sems,
):
    tp_count, ep_count = lax.axis_size("tp"), lax.axis_size("ep")
    tp_me, ep_me = lax.axis_index("tp"), lax.axis_index("ep")
    width = mix_ref.shape[1]
    column_tiles = width // LANES
    local_experts, capacity = main_out.shape[0], main_out.shape[2] + 1
    experts = local_experts * ep_count
    greet([{"tp": p} for p in axis_peers("tp")[1:]] + [{"ep": p} for p in axis_peers("ep")[1:]])
    loads = [
        pltpu.make_async_copy(hbm, vmem, load_sem.at[i])
        for i, (hbm, vmem) in enumerate(
            ((query_hbm, w_query), (key_hbm, w_key), (value_hbm, w_value))
        )
    ]
    for load in loads:
        load.start()

    normed = normalize(token_ref[...], token_gain_ref[...]).astype(BF16)
    main, last = slot_rows(ids_ref[...], experts, capacity)
    tokens = normed.shape[0]
    main_rows, last_rows = experts * (capacity - 1), experts * column_tiles
    slots = iota((main_rows, tokens), 0)
    hits = functools.reduce(jnp.add, [(slots == row).astype(F32) for row in main])
    main_send[...] = (
        matmul(hits.astype(BF16), normed).astype(BF16).reshape(main_send.shape)
    )
    slots = iota((last_rows, tokens), 0)
    tiles = jnp.zeros((last_rows, LANES), F32)
    for c in range(column_tiles):
        hits = [
            (slots == jnp.where(row >= 0, row * column_tiles + c, -1)).astype(F32) for row in last
        ]
        hits = functools.reduce(jnp.add, hits).astype(BF16)
        tiles = tiles + matmul(hits, normed[:, c * LANES : (c + 1) * LANES])
    last_send[...] = tiles.astype(BF16).reshape(last_send.shape)
    await_greetings(tp_count + ep_count - 2)
    copies = exchange_copies(
        "ep",
        (lambda e: main_send.at[e], lambda e: last_send.at[e]),
        (lambda e: main_out.at[:, e], lambda e: last_recv.at[e]),
        (main_sems.at[0], last_sems.at[0]),
        (main_sems.at[1], last_sems.at[1]),
    )
    for copy in copies:
        copy.start()

    normed = normalize(mix_ref[...], mix_gain_ref[...]).astype(BF16)
    rows = normed.shape[0]
    half = rows // 2
    pair_sums = iota((LANES, LANES), 0) // HEAD == iota((LANES, LANES), 1) // HEAD
    turned = head_turner(cosine_ref[...], sine_ref[...], pair_sums.astype(BF16))
    query_gain = jnp.concatenate([query_gain_ref[...]] * (LANES // HEAD), axis=1)
    key_gain = jnp.concatenate([key_gain_ref[...]] * (LANES // HEAD), axis=1)
    lower = iota((rows, LANES), 1) < HEAD
    lower_half = iota((half, LANES), 1) < HEAD
    for load in loads:
        load.wait()
    keys, values = matmul(normed, w_key[...]), matmul(normed, w_value[...])
    key_heads = w_key.shape[1] // HEAD
    group = tp_count // key_heads
    for t in range(key_heads // 2):
        key = turned(keys[:, t * LANES : (t + 1) * LANES], key_gain)
        value = values[:, t * LANES : (t + 1) * LANES].astype(BF16).astype(F32)
        for h, pairs in enumerate(
            (
                jnp.where(lower, key, pltpu.roll(value, HEAD, 1)),
                jnp.where(lower, pltpu.roll(key, HEAD, 1), value),
            )
        ):
            pairs = pairs.astype(BF16)
            for member in range(group):
                part = member % 2 * half
                head_send[(2 * t + h) * group + member, :half, :] = pairs[part : part + half]
    queries = matmul(normed, w_query[...])
    for t in range(tp_count // 2):
        tile = turned(queries[:, t * LANES : (t + 1) * LANES], query_gain)
        first, second = tile[:half], tile[half:]
        head_send[2 * t, half:, :] = jnp.where(
            lower_half, first, pltpu.roll(second, HEAD, 1)
        ).astype(BF16)
        head_send[2 * t + 1, half:, :] = jnp.where(
            lower_half, pltpu.roll(first, HEAD, 1), second
        ).astype(BF16)
    head_copies = exchange_copies(
        "tp",
        (lambda t: head_send.at[t],),
        (lambda t: head_out.at[t],),
        (head_sems.at[0],),
        (head_sems.at[1],),
    )
    for copy in head_copies:
        copy.start()

    head_out[tp_me] = head_send[tp_me]
    last_recv[ep_me] = last_send[ep_me]
    for j in range(local_experts):
        main_out[j, ep_me] = main_send[ep_me, j]
    for copy in copies:
        copy.wait()
    tiles = last_recv[...].reshape(last_rows, LANES)
    for j in range(local_experts):
        for c in range(column_tiles):
            chosen = pick(ep_count, last_rows, j * column_tiles + c, local_experts * column_tiles)
            last_out[j, :, c * LANES : (c + 1) * LANES] = matmul(chosen, tiles).astype(BF16)
    for copy in head_copies:
        copy.wait()


def dispatch(
    mix, mix_gain, w_query, w_key, w_value, query_gain, key_gain, cosine, sine, tokens, gain, ids,
    local_experts, capacity,
):
    tp_count, ep_count = lax.axis_size("tp"), lax.axis_size("ep")
    rows, width = mix.shape
    main = (capacity - 1, width)
    last = (ep_count, local_experts * width // LANES, LANES)
    head = (tp_count, rows, LANES)
    return pl.pallas_call(
        dispatch_body,
        out_shape=[
            jax.ShapeDtypeStruct(head, BF16),
            jax.ShapeDtypeStruct((local_experts, ep_count) + main, BF16),
            jax.ShapeDtypeStruct((local_experts, ep_count, width), BF16),
        ],
        in_specs=[VMEM_SPEC] * 2 + [HBM_SPEC] * 3 + [VMEM_SPEC] * 7,
        out_specs=[VMEM_SPEC] * 3,
        scratch_shapes=[
            pltpu.VMEM(w_query.shape, BF16),
            pltpu.VMEM(w_key.shape, BF16),
            pltpu.VMEM(w_value.shape, BF16),
            pltpu.VMEM(head, BF16),
            pltpu.VMEM((ep_count, local_experts) + main, BF16),
            pltpu.VMEM(last, BF16),
            pltpu.VMEM(last, BF16),
            DMA((3,)),
            DMA((2, tp_count)),
            DMA((2, ep_count)),
            DMA((2, ep_count)),
        ],
        name="dispatch",
        compiler_params=pltpu.CompilerParams(
            collective_id=0, has_side_effects=True, vmem_limit_bytes=63 * MIB
        ),
    )(mix, mix_gain, w_query, w_key, w_value, query_gain, key_gain, cosine, sine, tokens, gain, ids)


def ring_places():
    me = lax.axis_index("tp")
    chips = lax.axis_size("tp") // 2
    chip, core = me // 2, lax.rem(me, 2)
    ahead = lax.rem(chip + 1 - 2 * core + chips, chips) * 2 + core
    behind = lax.rem(chip - 1 + 2 * core + chips, chips) * 2 + core
    partner = chip * 2 + 1 - core
    return core, {"tp": ahead}, {"tp": behind}, {"tp": partner}


def gather_body(
    head_ref,
    main_ref,
    last_ref,
    gate_hbm,
    up_hbm,
    down_hbm,
    own_out,
    pair_out,
    keys_out,
    gate,
    up,
    down,
    held,
    own_part,
    pair_part,
    load_sem,
    key_sem,
    ring_sems,
    pair_sems,
    own_sem,
    part_sems,
    key_sems,
    share_sems,
):
    pieces, _, piece_rows, width = held.shape
    core, ahead, behind, partner = ring_places()
    ep_me, ep_count = lax.axis_index("ep"), lax.axis_size("ep")
    greet([ahead, behind, partner] + [{"ep": p} for p in axis_peers("ep")[1:]])
    loads = [
        pltpu.make_async_copy(hbm, vmem, load_sem.at[i])
        for i, (hbm, vmem) in enumerate(((gate_hbm, gate), (up_hbm, up), (down_hbm, down)))
    ]
    for load in loads:
        load.start()
    tail_rows = last_ref.shape[1]
    for j in range(2):
        held[j, 0, : piece_rows - tail_rows, :] = main_ref[j].reshape(
            piece_rows - tail_rows, width
        )
        held[j, 0, piece_rows - tail_rows :, :] = last_ref[j]

    def ring_copy(i):
        return remote(
            held.at[i, 0], held.at[i + 2, 0], ring_sems.at[0, i], ring_sems.at[1, i], ahead
        )

    def pair_copy(i):
        return remote(
            held.at[i, 0], held.at[i, 1], pair_sems.at[0, i], pair_sems.at[1, i], partner
        )

    def part_copy(i):
        return remote(
            pair_part.at[i], pair_out.at[i], part_sems.at[0, i], part_sems.at[1, i], partner
        )

    def own_copy(i):
        return pltpu.make_async_copy(own_part.at[i], own_out.at[i], own_sem.at[i])

    half = head_ref.shape[1] // 2
    own_keys = head_ref.at[:, pl.ds(0, half), :]
    key_copies = exchange_copies(
        "ep",
        (lambda e: own_keys,),
        (lambda e: keys_out.at[core, e],),
        (key_sems.at[0],),
        (key_sems.at[1],),
    )
    keep_keys = pltpu.make_async_copy(own_keys, keys_out.at[core, ep_me], key_sem.at[0])

    def share(source, d):
        origin = lax.rem(ep_me - d + ep_count, ep_count)
        target = keys_out.at[core, origin]
        return remote(
            target if source is None else source,
            target,
            share_sems.at[0, d],
            share_sems.at[1, d],
            partner,
        )

    def key_arrival(d):
        target = keys_out.at[core, lax.rem(ep_me - d + ep_count, ep_count)]
        return remote(target, target, key_sems.at[0, d], key_sems.at[1, d], partner)

    await_greetings(ep_count + 2)

    def step(i, _):
        @pl.when(i < pieces)
        def _():
            @pl.when(i >= 2)
            def _():
                ring_copy(i - 2).wait_recv()

            @pl.when(i < pieces - 2)
            def _():
                ring_copy(i).start()

            pair_copy(i).start()

        @pl.when(i == 1)
        def _():
            for copy in key_copies:
                copy.start()
            keep_keys.start()
            share(own_keys, 0).start()
            for load in loads:
                load.wait()

        @pl.when(i >= 3)
        def _():
            key_arrival(i - 2).wait_recv()
            share(None, i - 2).start()

        @pl.when(jnp.logical_and(i >= 1, i <= pieces))
        def _():
            piece = i - 1
            expert = lax.rem(piece, 2)
            pair_copy(piece).wait_recv()
            rows = held[piece].reshape(2 * piece_rows, width)
            gate_act = matmul(rows, gate[expert])
            up_act = matmul(rows, up[expert])
            hidden = (gate_act / (1.0 + jnp.exp(-gate_act)) * up_act).astype(BF16)
            sums = matmul(hidden, down[expert]).astype(BF16)
            own_part[piece] = sums[:piece_rows]
            pair_part[piece] = sums[piece_rows:]

        @pl.when(i >= 2)
        def _():
            own_copy(i - 2).start()
            part_copy(i - 2).start()

        return 0

    lax.fori_loop(0, pieces + 2, step, 0)

    def finish(i, _):
        @pl.when(i < pieces - 2)
        def _():
            ring_copy(i).wait_send()

        pair_copy(i).wait_send()
        own_copy(i).wait()
        part_copy(i).wait()
        return 0

    lax.fori_loop(0, pieces, finish, 0)
    keep_keys.wait()
    for copy in key_copies:
        copy.wait_send()

    def finish_share(d, _):
        share(None, d).wait()
        return 0

    lax.fori_loop(0, ep_count, finish_share, 0)


def gather_experts(head, main, last, w_gate, w_up, w_down):
    pieces, ep_count = lax.axis_size("tp"), lax.axis_size("ep")
    piece_rows, width = ep_count * (main.shape[2] + 1), main.shape[3]
    part = (pieces, piece_rows, width)
    keys = (2, ep_count, pieces, head.shape[1] // 2, LANES)
    assert pieces == ep_count
    return pl.pallas_call(
        gather_body,
        out_shape=[jax.ShapeDtypeStruct(shape, BF16) for shape in (part, part, keys)],
        in_specs=[VMEM_SPEC] * 3 + [HBM_SPEC] * 3,
        out_specs=[HBM_SPEC] * 3,
        scratch_shapes=[
            pltpu.VMEM(w_gate.shape, BF16),
            pltpu.VMEM(w_up.shape, BF16),
            pltpu.VMEM(w_down.shape, BF16),
            pltpu.VMEM((pieces, 2, piece_rows, width), BF16),
            pltpu.VMEM(part, BF16),
            pltpu.VMEM(part, BF16),
            DMA((3,)),
            DMA((1,)),
            DMA((2, pieces)),
            DMA((2, pieces)),
            DMA((pieces,)),
            DMA((2, pieces)),
            DMA((2, ep_count)),
            DMA((2, ep_count)),
        ],
        name="gather_experts",
        compiler_params=pltpu.CompilerParams(
            collective_id=1, has_side_effects=True, vmem_limit_bytes=63 * MIB
        ),
    )(head, main, last, w_gate, w_up, w_down)


def scatter_body(
    query_tile,
    key_block,
    head_ref,
    keys_hbm,
    own_hbm,
    part_hbm,
    main_out,
    last_out,
    mixed_out,
    queries,
    pairs,
    own_part,
    pair_part,
    arrived,
    leaving,
    row_max,
    row_sum,
    row_acc,
    key_sem,
    own_sem,
    part_sem,
    ring_sems,
):
    pieces, piece_rows, width = own_part.shape
    groups, rows, _ = head_ref.shape
    half = rows // 2
    tiles, blocks = groups * rows // query_tile, pairs.shape[0] // key_block
    slices = tiles * blocks // pieces
    tile_groups = query_tile // rows
    main_rows = piece_rows - last_out.shape[1]
    _, ahead, behind, _ = ring_places()
    greet([ahead, behind])

    def loads(i):
        slot = lax.rem(i + 2, pieces)
        return (
            pltpu.make_async_copy(own_hbm.at[slot], own_part.at[i], own_sem.at[i]),
            pltpu.make_async_copy(part_hbm.at[slot], pair_part.at[i], part_sem.at[i]),
        )

    def key_load(block):
        chosen = pl.ds(pl.multiple_of(block * key_block, key_block), key_block)
        return pltpu.make_async_copy(keys_hbm.at[chosen, :], pairs.at[chosen, :], key_sem.at[block])

    def ring_copy(i):
        return remote(leaving.at[i], arrived.at[i], ring_sems.at[0, i], ring_sems.at[1, i], ahead)

    def start_loads(i, _):
        for load in loads(i):
            load.start()

        @pl.when(i < blocks)
        def _():
            key_load(i).start()

        return 0

    lax.fori_loop(0, pieces, start_loads, 0)
    packed = head_ref[:, half:, :].astype(F32).reshape(groups * half, LANES)
    lower = iota(packed.shape, 1) < HEAD
    for h, values in enumerate((packed, pltpu.roll(packed, HEAD, 1))):
        values = jnp.where(lower, values, 0.0).astype(BF16).reshape(groups, half, LANES)
        queries[:, h * half : (h + 1) * half, :] = values
    row_max[...] = jnp.full(row_max.shape, -1e30, F32)
    row_sum[...] = jnp.zeros(row_sum.shape, F32)
    row_acc[...] = jnp.zeros(row_acc.shape, F32)
    await_greetings(2)

    def attend_slice(number):
        block, tile = number // tiles, lax.rem(number, tiles)
        chosen = queries[pl.ds(tile * tile_groups, tile_groups)].reshape(query_tile, LANES)
        keys = pairs[pl.ds(pl.multiple_of(block * key_block, key_block), key_block), :]
        scores = lax.dot_general(
            chosen, keys, (((1,), (1,)), ((), ())), preferred_element_type=F32
        )
        old_max = row_max[tile][:, :1]
        new_max = jnp.maximum(old_max, jnp.max(scores, axis=1, keepdims=True))
        shrink = jnp.exp2((old_max - new_max) * EXP2_SCALE)
        raised = jnp.exp2((scores - new_max) * EXP2_SCALE)
        lane_sums = raised[:, :LANES]
        for lane in range(LANES, key_block, LANES):
            lane_sums = lane_sums + raised[:, lane : lane + LANES]
        row_max[tile] = jnp.broadcast_to(new_max, (query_tile, LANES))
        row_sum[tile] = row_sum[tile] * shrink + lane_sums
        row_acc[tile] = row_acc[tile] * shrink + matmul(raised.astype(BF16), keys)

    def step(i, _):
        for load in loads(i):
            load.wait()

        @pl.when(i < 2)
        def _():
            total = own_part[i].astype(F32) + pair_part[i].astype(F32)
            leaving[i] = total.astype(BF16)

        @pl.when(i >= 2)
        def _():
            ring_copy(i - 2).wait_recv()
            total = own_part[i].astype(F32) + pair_part[i].astype(F32)
            total = (total + arrived[i - 2].astype(F32)).astype(BF16)

            @pl.when(i < pieces - 2)
            def _():
                leaving[i] = total

            @pl.when(i >= pieces - 2)
            def _():
                j = i - (pieces - 2)
                main_out[j] = total[:main_rows].reshape(main_out.shape[1:])
                last_out[j] = total[main_rows:]

        @pl.when(i < pieces - 2)
        def _():
            ring_copy(i).start()

        @pl.when(lax.rem(i * slices, tiles) == 0)
        def _():
            key_load(i * slices // tiles).wait()

        for part in range(slices):
            attend_slice(i * slices + part)
        return 0

    lax.fori_loop(0, pieces, step, 0)

    def finish(i, _):
        ring_copy(i).wait_send()
        return 0

    lax.fori_loop(0, pieces - 2, finish, 0)
    for tile in range(tiles):
        mixed = row_acc[tile] / jnp.sum(row_sum[tile], axis=1, keepdims=True)
        mixed_out[tile * tile_groups : (tile + 1) * tile_groups] = mixed.astype(BF16).reshape(
            tile_groups, rows, LANES
        )


def scatter_experts(head, keys, own_part, pair_part, capacity):
    pieces, piece_rows, width = own_part.shape
    groups, rows, _ = head.shape
    key_count = keys.shape[0]
    query_tile, key_block = math.gcd(groups * rows, 256), math.gcd(key_count, 2048)
    tiles = groups * rows // query_tile
    ep_count = piece_rows // capacity
    state = pltpu.VMEM((tiles, query_tile, LANES), F32)
    return pl.pallas_call(
        functools.partial(scatter_body, query_tile, key_block),
        out_shape=[
            jax.ShapeDtypeStruct((2, ep_count, capacity - 1, width), BF16),
            jax.ShapeDtypeStruct((2, ep_count, width), BF16),
            jax.ShapeDtypeStruct(head.shape, BF16),
        ],
        in_specs=[VMEM_SPEC] + [HBM_SPEC] * 3,
        out_specs=[VMEM_SPEC] * 3,
        scratch_shapes=[
            pltpu.VMEM(head.shape, BF16),
            pltpu.VMEM(keys.shape, BF16),
            pltpu.VMEM((pieces, piece_rows, width), BF16),
            pltpu.VMEM((pieces, piece_rows, width), BF16),
            pltpu.VMEM((pieces - 2, piece_rows, width), BF16),
            pltpu.VMEM((pieces - 2, piece_rows, width), BF16),
            state,
            state,
            state,
            DMA((key_count // key_block,)),
            DMA((pieces,)),
            DMA((pieces,)),
            DMA((2, pieces - 2)),
        ],
        name="scatter_experts",
        compiler_params=pltpu.CompilerParams(
            collective_id=2, has_side_effects=True, vmem_limit_bytes=63 * MIB
        ),
    )(head, keys, own_part, pair_part)


def collect_body(
    main_ref,
    last_ref,
    mixed_ref,
    out_hbm,
    ids_ref,
    weights_ref,
    mix_out,
    experts_out,
    w_out,
    results,
    last_send,
    last_recv,
    main_recv,
    mixed_recv,
    load_sem,
    head_sems,
    main_sems,
    last_sems,
):
    tp_count, ep_count = lax.axis_size("tp"), lax.axis_size("ep")
    tp_me, ep_me = lax.axis_index("tp"), lax.axis_index("ep")
    local_experts, _, main_cap, width = main_ref.shape
    column_tiles = width // LANES
    experts = local_experts * ep_count
    main_rows, last_rows = experts * main_cap, experts * column_tiles
    greet([{"tp": p} for p in axis_peers("tp")[1:]] + [{"ep": p} for p in axis_peers("ep")[1:]])
    load = pltpu.make_async_copy(out_hbm, w_out, load_sem.at[0])
    load.start()
    tiles = jnp.zeros((last_rows, LANES), F32)
    for j in range(local_experts):
        for c in range(column_tiles):
            spot = place(last_rows, ep_count, j * column_tiles + c, local_experts * column_tiles)
            tiles = tiles + matmul(spot, last_ref[j, :, c * LANES : (c + 1) * LANES])
    last_send[...] = tiles.astype(BF16).reshape(last_send.shape)
    await_greetings(tp_count + ep_count - 2)
    copies = exchange_copies(
        "ep",
        (lambda e: main_ref.at[:, e], lambda e: last_send.at[e]),
        (lambda e: main_recv.at[e], lambda e: last_recv.at[e]),
        (main_sems.at[0], last_sems.at[0]),
        (main_sems.at[1], last_sems.at[1]),
    )
    head_copies = exchange_copies(
        "tp",
        (lambda t: mixed_ref.at[t],),
        (lambda t: mixed_recv.at[t],),
        (head_sems.at[0],),
        (head_sems.at[1],),
    )
    for copy in head_copies + copies:
        copy.start()
    mixed_recv[tp_me] = mixed_ref[tp_me]
    last_recv[ep_me] = last_send[ep_me]
    for j in range(local_experts):
        main_recv[ep_me, j] = main_ref[j, ep_me]

    main, last = slot_rows(ids_ref[...], experts, main_cap + 1)
    tokens = ids_ref.shape[1]
    takers = []
    for k in range(len(main)):
        slot = jnp.where(main[k] >= 0, main[k], jnp.where(last[k] >= 0, last[k] + main_rows, -1))
        spot = (iota((results.shape[0], tokens), 0) == slot).astype(F32)
        takers.append(jnp.transpose(spot).astype(BF16))
    load.wait()
    for copy in head_copies:
        copy.wait()
    lower = iota((mixed_recv.shape[1], LANES), 1) < HEAD
    heads = []
    for t in range(tp_count // 2):
        even, odd = mixed_recv[2 * t].astype(F32), mixed_recv[2 * t + 1].astype(F32)
        heads.append(jnp.where(lower, pltpu.roll(even, HEAD, 1), odd).astype(BF16))
    mix_out[...] = matmul(jnp.concatenate(heads, axis=1), w_out[...]).astype(BF16)

    for copy in copies:
        copy.wait()
    results[:main_rows, :] = main_recv[...].reshape(main_rows, width)
    results[main_rows:, :] = jnp.zeros((results.shape[0] - main_rows, width), BF16)
    tiles = last_recv[...].reshape(last_rows, LANES)
    for c in range(column_tiles):
        chosen = matmul(pick(experts, last_rows, c, column_tiles), tiles)
        results[main_rows : main_rows + experts, c * LANES : (c + 1) * LANES] = chosen.astype(BF16)
    combined = jnp.zeros((tokens, width), F32)
    for k, taker in enumerate(takers):
        combined = combined + weights_ref[:, k : k + 1] * matmul(taker, results[...])
    experts_out[...] = combined.astype(BF16)


def collect(main, last, mixed, w_out, ids, weights):
    tp_count, ep_count = lax.axis_size("tp"), lax.axis_size("ep")
    local_experts, _, main_cap, width = main.shape
    experts = local_experts * ep_count
    result_rows = -(-experts * (main_cap + 1) // LANES) * LANES
    tiles = (ep_count, local_experts * width // LANES, LANES)
    return pl.pallas_call(
        collect_body,
        out_shape=[
            jax.ShapeDtypeStruct((mixed.shape[1], w_out.shape[1]), BF16),
            jax.ShapeDtypeStruct((ids.shape[1], width), BF16),
        ],
        in_specs=[VMEM_SPEC] * 3 + [HBM_SPEC] + [VMEM_SPEC] * 2,
        out_specs=[VMEM_SPEC] * 2,
        scratch_shapes=[
            pltpu.VMEM(w_out.shape, BF16),
            pltpu.VMEM((result_rows, width), BF16),
            pltpu.VMEM(tiles, BF16),
            pltpu.VMEM(tiles, BF16),
            pltpu.VMEM((ep_count, local_experts, main_cap, width), BF16),
            pltpu.VMEM(mixed.shape, BF16),
            DMA((1,)),
            DMA((2, tp_count)),
            DMA((2, ep_count)),
            DMA((2, ep_count)),
        ],
        name="collect",
        compiler_params=pltpu.CompilerParams(
            collective_id=3, has_side_effects=True, vmem_limit_bytes=63 * MIB
        ),
    )(main, last, mixed, w_out, ids, weights)


def body(
    mix_tokens,
    mix_gain,
    w_query,
    w_key,
    w_value,
    query_gain,
    key_gain,
    w_out,
    expert_tokens,
    expert_gain,
    route_ids,
    route_weights,
    w_gate,
    w_up,
    w_down,
):
    tp_count, ep_count = lax.axis_size("tp"), lax.axis_size("ep")
    seq_rows, _, model_width = mix_tokens.shape
    tok_count, top_count = route_ids.shape
    local_experts = w_gate.shape[0]
    capacity = tok_count * top_count * 9 // (8 * local_experts * ep_count)
    first = (lax.axis_index("ep") * tp_count + lax.axis_index("tp")) * seq_rows
    cosine, sine = lane_tables(first + jnp.arange(seq_rows, dtype=jnp.int32))
    id_rows = jnp.transpose(route_ids)
    head, main, last = dispatch(
        mix_tokens.reshape(seq_rows, model_width),
        mix_gain.reshape(1, model_width),
        w_query,
        w_key,
        w_value,
        query_gain.reshape(1, HEAD),
        key_gain.reshape(1, HEAD),
        cosine,
        sine,
        expert_tokens,
        expert_gain.reshape(1, model_width),
        id_rows,
        local_experts,
        capacity,
    )
    own_part, pair_part, keys = gather_experts(head, main, last, w_gate, w_up, w_down)
    keys = keys.reshape(-1, LANES)
    main, last, mixed = scatter_experts(head, keys, own_part, pair_part, capacity)
    mix_out, experts_out = collect(main, last, mixed, w_out, id_rows, route_weights)
    return (mix_out[:, None, :], experts_out)


def solution(mesh):
    placed = (
        P(("ep", "tp"), None, None),
        P(),
        P(),
        P(),
        P(),
        P(),
        P(),
        P(),
        P(("ep", "tp"), None),
        P(),
        P(("ep", "tp"), None),
        P(("ep", "tp"), None),
        P("ep", None, "tp"),
        P("ep", None, "tp"),
        P("ep", "tp", None),
    )
    return jax.shard_map(
        body,
        mesh=mesh,
        in_specs=placed,
        out_specs=(P(("ep", "tp"), None, None), P(("ep", "tp"), None)),
        check_vma=False,
    )
```

```python
import functools
import math

import jax
import jax.numpy as jnp
from jax import lax
from jax.experimental import pallas as pl
from jax.experimental.pallas import tpu as pltpu
import numpy as np
from jax.sharding import PartitionSpec as P

HEAD = 64
GRID_W = 64
LANES = 128
KEY_GROUPS = 4
EXP2_SCALE = HEAD ** (-0.5) * math.log2(math.e)
MESH = pl.DeviceIdType.MESH
MIB = 1024 * 1024
BF16, F32 = jnp.bfloat16, jnp.float32
VMEM_SPEC = pl.BlockSpec(memory_space=pltpu.VMEM)
HBM_SPEC = pl.BlockSpec(memory_space=pltpu.HBM)
DMA = pltpu.SemaphoreType.DMA


epsilon = 1e-06


def normalize(values, gain_vec):
    widened = values.astype(F32)
    return (
        widened
        * lax.rsqrt(jnp.mean(widened * widened, axis=-1, keepdims=True) + epsilon)
        * gain_vec
    )


def matmul(left, right):
    return jnp.dot(left, right, preferred_element_type=F32)


def frequencies():
    quarter = HEAD // 4
    powers = np.float32(10000.0) ** (-np.arange(quarter, dtype=np.float32) / np.float32(quarter))
    return np.tile(powers.astype(np.float32), LANES // quarter).reshape(1, LANES)


def greet(peers):
    barrier = pltpu.get_barrier_semaphore()
    for peer in peers:
        pl.semaphore_signal(barrier, inc=1, device_id=peer, device_id_type=MESH)


def await_greetings(count):
    pl.semaphore_wait(pltpu.get_barrier_semaphore(), count)


def axis_peers(axis):
    me, count = lax.axis_index(axis), lax.axis_size(axis)
    return [lax.rem(me + d, count) for d in range(count)]


def remote(source, target, send_sem, recv_sem, device_id):
    return pltpu.make_async_remote_copy(
        src_ref=source,
        dst_ref=target,
        send_sem=send_sem,
        recv_sem=recv_sem,
        device_id=device_id,
        device_id_type=MESH,
    )


def exchange_copies(axis, sources, targets, sends, recvs):
    me = lax.axis_index(axis)
    return [
        remote(source(peer), target(me), send.at[d], recv.at[d], {axis: peer})
        for d, peer in enumerate(axis_peers(axis))
        if d > 0
        for source, target, send, recv in zip(sources, targets, sends, recvs)
    ]


def iota(shape, axis):
    return lax.broadcasted_iota(jnp.int32, shape, axis)


def slot_rows(id_rows, experts, capacity):
    choices, tokens = id_rows.shape
    marks = [
        (iota((experts, tokens), 0) == id_rows[k : k + 1, :]).astype(F32) for k in range(choices)
    ]
    earlier = (iota((tokens, tokens), 0) < iota((tokens, tokens), 1)).astype(BF16)
    ranks = matmul(functools.reduce(jnp.add, marks).astype(BF16), earlier)
    main, last = [], []
    for k in range(choices):
        rank = jnp.sum(marks[k] * ranks, axis=0, keepdims=True).astype(jnp.int32)
        ids = id_rows[k : k + 1, :]
        main.append(jnp.where(rank < capacity - 1, ids * (capacity - 1) + rank, -1))
        last.append(jnp.where(rank == capacity - 1, ids, -1))
    return main, last


def pick(rows, columns, first, stride):
    wanted = iota((rows, columns), 0) * stride + first
    return (iota((rows, columns), 1) == wanted).astype(BF16)


def place(rows, columns, first, stride):
    wanted = iota((rows, columns), 1) * stride + first
    return (iota((rows, columns), 0) == wanted).astype(BF16)


def head_turner(first, rows, powers, pair_sums):
    lane = iota((rows, LANES), 1)
    quarter = HEAD // 4
    position = first + iota((rows, LANES), 0)
    by_row = lax.rem(lane, HEAD) < HEAD // 2
    place = jnp.where(by_row, position // GRID_W, lax.rem(position, GRID_W)).astype(F32)
    angles = place * powers
    cosine = jnp.cos(angles)
    sine = jnp.sin(angles)
    sine = jnp.where(lax.rem(lane, 2 * quarter) < quarter, -sine, sine)

    def turned(raw, gain):
        values = raw.astype(BF16).astype(F32)
        squares = values * values
        high = squares.astype(BF16)
        low = (squares - high.astype(F32)).astype(BF16)
        sums = matmul(high, pair_sums) + matmul(low, pair_sums)
        values = values * lax.rsqrt(sums * (1.0 / HEAD) + epsilon) * gain
        partner = jnp.where(
            lax.rem(lane, 2 * quarter) < quarter,
            pltpu.roll(values, LANES - quarter, 1),
            pltpu.roll(values, quarter, 1),
        )
        return (values * cosine + partner * sine).astype(BF16).astype(F32)

    return turned


def ring_places():
    me = lax.axis_index("tp")
    chips = lax.axis_size("tp") // 2
    chip, core = me // 2, lax.rem(me, 2)
    ahead = lax.rem(chip + 1 - 2 * core + chips, chips) * 2 + core
    behind = lax.rem(chip - 1 + 2 * core + chips, chips) * 2 + core
    partner = chip * 2 + 1 - core
    return core, {"tp": ahead}, {"tp": behind}, {"tp": partner}


def layer_body(
    mix_ref,
    mix_gain_ref,
    query_hbm,
    key_hbm,
    value_hbm,
    query_gain_ref,
    key_gain_ref,
    powers_ref,
    out_hbm,
    token_ref,
    token_gain_ref,
    ids_ref,
    weights_ref,
    gate_hbm,
    up_hbm,
    down_hbm,
    mix_out,
    experts_out,
    w_query,
    w_key,
    w_value,
    w_out,
    gate,
    up,
    down,
    head_send,
    head_recv,
    main_send,
    main_in,
    last_send,
    last_in,
    held,
    own_part,
    pair_part,
    pair_in,
    leaving,
    arrived,
    keys,
    queries,
    row_max,
    row_sum,
    row_acc,
    mixed_send,
    mixed_recv,
    main_back,
    main_recv,
    last_back,
    last_recv,
    results,
    load_sem,
    head_sems,
    main_sems,
    last_sems,
    ring_sems,
    pair_sems,
    part_sems,
    sum_sems,
    key_sems,
    share_sems,
    mixed_sems,
    main_back_sems,
    last_back_sems,
):
    tp_count, ep_count = lax.axis_size("tp"), lax.axis_size("ep")
    tp_me, ep_me = lax.axis_index("tp"), lax.axis_index("ep")
    core, ahead, behind, partner = ring_places()
    greet([{"tp": p} for p in axis_peers("tp")[1:]] + [{"ep": p} for p in axis_peers("ep")[1:]])
    loads = [
        pltpu.make_async_copy(hbm, vmem, load_sem.at[i])
        for i, (hbm, vmem) in enumerate(
            (
                (query_hbm, w_query),
                (key_hbm, w_key),
                (value_hbm, w_value),
                (gate_hbm, gate),
                (up_hbm, up),
                (down_hbm, down),
                (out_hbm, w_out),
            )
        )
    ]
    for load in loads:
        load.start()

    local_experts, _, main_cap, width = main_in.shape
    column_tiles = width // LANES
    experts = local_experts * ep_count
    capacity = main_cap + 1
    tokens = token_ref.shape[0]
    main_rows, last_rows = experts * main_cap, experts * column_tiles
    normed = normalize(token_ref[...], token_gain_ref[...]).astype(BF16)
    main, last = slot_rows(ids_ref[...], experts, capacity)
    slots = iota((main_rows, tokens), 0)
    hits = functools.reduce(jnp.add, [(slots == row).astype(F32) for row in main])
    main_send[...] = matmul(hits.astype(BF16), normed).astype(BF16).reshape(main_send.shape)
    slots = iota((last_rows, tokens), 0)
    tiles = jnp.zeros((last_rows, LANES), F32)
    for c in range(column_tiles):
        hits = [
            (slots == jnp.where(row >= 0, row * column_tiles + c, -1)).astype(F32) for row in last
        ]
        hits = functools.reduce(jnp.add, hits).astype(BF16)
        tiles = tiles + matmul(hits, normed[:, c * LANES : (c + 1) * LANES])
    last_send[...] = tiles.astype(BF16).reshape(last_send.shape)
    await_greetings(tp_count + ep_count - 2)
    row_copies = exchange_copies(
        "ep",
        (lambda e: main_send.at[e], lambda e: last_send.at[e]),
        (lambda e: main_in.at[:, e], lambda e: last_in.at[e]),
        (main_sems.at[0], last_sems.at[0]),
        (main_sems.at[1], last_sems.at[1]),
    )
    for copy in row_copies:
        copy.start()

    normed = normalize(mix_ref[...], mix_gain_ref[...]).astype(BF16)
    rows = normed.shape[0]
    half = rows // 2
    pair_sums = iota((LANES, LANES), 0) // HEAD == iota((LANES, LANES), 1) // HEAD
    turned = head_turner(
        (ep_me * tp_count + tp_me) * rows, rows, powers_ref[...], pair_sums.astype(BF16)
    )
    query_gain = jnp.concatenate([query_gain_ref[...]] * (LANES // HEAD), axis=1)
    key_gain = jnp.concatenate([key_gain_ref[...]] * (LANES // HEAD), axis=1)
    lower = iota((rows, LANES), 1) < HEAD
    lower_half = iota((half, LANES), 1) < HEAD
    for load in loads[:3]:
        load.wait()
    raw_keys, raw_values = matmul(normed, w_key[...]), matmul(normed, w_value[...])
    key_heads = w_key.shape[1] // HEAD
    group = tp_count // key_heads
    for t in range(key_heads // 2):
        key = turned(raw_keys[:, t * LANES : (t + 1) * LANES], key_gain)
        value = raw_values[:, t * LANES : (t + 1) * LANES].astype(BF16).astype(F32)
        for h, pairs in enumerate(
            (
                jnp.where(lower, key, pltpu.roll(value, HEAD, 1)),
                jnp.where(lower, pltpu.roll(key, HEAD, 1), value),
            )
        ):
            pairs = pairs.astype(BF16)
            for member in range(group):
                part = member % 2 * half
                head_send[(2 * t + h) * group + member, :half, :] = pairs[part : part + half]
    raw_queries = matmul(normed, w_query[...])
    for t in range(tp_count // 2):
        tile = turned(raw_queries[:, t * LANES : (t + 1) * LANES], query_gain)
        first, second = tile[:half], tile[half:]
        head_send[2 * t, half:, :] = jnp.where(
            lower_half, first, pltpu.roll(second, HEAD, 1)
        ).astype(BF16)
        head_send[2 * t + 1, half:, :] = jnp.where(
            lower_half, pltpu.roll(first, HEAD, 1), second
        ).astype(BF16)
    head_copies = exchange_copies(
        "tp",
        (lambda t: head_send.at[t],),
        (lambda t: head_recv.at[t],),
        (head_sems.at[0],),
        (head_sems.at[1],),
    )
    for copy in head_copies:
        copy.start()
    head_recv[tp_me] = head_send[tp_me]
    last_in[ep_me] = last_send[ep_me]
    for j in range(local_experts):
        main_in[j, ep_me] = main_send[ep_me, j]
    row_max[...] = jnp.full(row_max.shape, -1e30, F32)
    row_sum[...] = jnp.zeros(row_sum.shape, F32)
    row_acc[...] = jnp.zeros(row_acc.shape, F32)

    pieces, _, piece_rows, _ = held.shape
    held_main = ep_count * main_cap
    for copy in row_copies:
        copy.wait_recv()
    tiles = last_in[...].reshape(last_rows, LANES)
    for j in range(local_experts):
        held[j, 0, :held_main, :] = main_in[j].reshape(held_main, width)
        for c in range(column_tiles):
            chosen = pick(ep_count, last_rows, j * column_tiles + c, local_experts * column_tiles)
            held[j, 0, held_main:, c * LANES : (c + 1) * LANES] = matmul(chosen, tiles).astype(BF16)
    def ring_copy(i):
        return remote(
            held.at[i, 0], held.at[i + 2, 0], ring_sems.at[0, i], ring_sems.at[1, i], ahead
        )

    def pair_copy(i):
        return remote(
            held.at[i, 0], held.at[i, 1], pair_sems.at[0, i], pair_sems.at[1, i], partner
        )

    def part_copy(i):
        return remote(
            pair_part.at[i], pair_in.at[i], part_sems.at[0, i], part_sems.at[1, i], partner
        )

    def sum_copy(m):
        return remote(leaving.at[m], arrived.at[m], sum_sems.at[0, m], sum_sems.at[1, m], ahead)

    own_keys = head_recv.at[:, pl.ds(0, half), :]
    key_copies = [
        remote(
            own_keys, keys.at[core, d], key_sems.at[0, d], key_sems.at[1, d], {"ep": peer}
        )
        for d, peer in enumerate(axis_peers("ep"))
        if d > 0
    ]

    def key_arrival(d):
        return remote(
            keys.at[core, d], keys.at[core, d], key_sems.at[0, d], key_sems.at[1, d], partner
        )

    def share(d):
        return remote(
            keys.at[core, d], keys.at[core, d], share_sems.at[0, d], share_sems.at[1, d], partner
        )

    tiles_count, tile_rows, _ = row_acc.shape
    tile_groups = tile_rows // rows
    groups = tp_count
    key_group = ep_count // KEY_GROUPS
    key_rows = key_group * groups * half

    def attend_slice(tile, block):
        chosen = queries[tile * tile_groups : (tile + 1) * tile_groups].reshape(tile_rows, LANES)
        pairs = keys[lax.rem(block, 2), pl.ds(block // 2 * key_group, key_group)]
        pairs = pairs.reshape(key_rows, LANES)
        scores = lax.dot_general(
            chosen, pairs, (((1,), (1,)), ((), ())), preferred_element_type=F32
        )
        old_max = row_max[tile][:, :1]
        new_max = jnp.maximum(old_max, jnp.max(scores, axis=1, keepdims=True))
        shrink = jnp.exp2((old_max - new_max) * EXP2_SCALE)
        raised = jnp.exp2((scores - new_max) * EXP2_SCALE)
        lane_sums = raised[:, :LANES]
        for lane in range(LANES, key_rows, LANES):
            lane_sums = lane_sums + raised[:, lane : lane + LANES]
        row_max[tile] = jnp.broadcast_to(new_max, (tile_rows, LANES))
        row_sum[tile] = row_sum[tile] * shrink + lane_sums
        row_acc[tile] = row_acc[tile] * shrink + matmul(raised.astype(BF16), pairs)

    def step(i, _):
        @pl.when(jnp.logical_and(i >= 2, i < pieces + 2))
        def _():
            part_copy(i - 2).start()

        @pl.when(i < pieces)
        def _():
            @pl.when(i >= 2)
            def _():
                ring_copy(i - 2).wait_recv()

            @pl.when(i < pieces - 2)
            def _():
                ring_copy(i).start()

            pair_copy(i).start()

        @pl.when(i == 1)
        def _():
            for load in loads[3:]:
                load.wait()

        @pl.when(i == 2)
        def _():
            for copy in head_copies:
                copy.wait_recv()
            for copy in key_copies:
                copy.start()
            keys[core, 0] = head_recv[:, :half, :]
            packed = head_recv[:, half:, :].astype(F32).reshape(groups * half, LANES)
            lower_lanes = iota(packed.shape, 1) < HEAD
            for h, values in enumerate((packed, pltpu.roll(packed, HEAD, 1))):
                values = jnp.where(lower_lanes, values, 0.0).astype(BF16)
                queries[:, h * half : (h + 1) * half, :] = values.reshape(groups, half, LANES)

        @pl.when(jnp.logical_and(i >= 4, i < 4 + KEY_GROUPS))
        def _():
            for g in range(key_group):
                d = (i - 4) * key_group + g

                @pl.when(d > 0)
                def _():
                    key_arrival(d).wait_recv()

                share(d).start()

        @pl.when(jnp.logical_and(i >= 1, i <= pieces))
        def _():
            piece = i - 1
            expert = lax.rem(piece, 2)
            pair_copy(piece).wait_recv()
            values = held[piece].reshape(2 * piece_rows, width)
            gate_act = matmul(values, gate[expert])
            up_act = matmul(values, up[expert])
            hidden = (gate_act / (1.0 + jnp.exp(-gate_act)) * up_act).astype(BF16)
            sums = matmul(hidden, down[expert]).astype(BF16)
            own_part[piece] = sums[:piece_rows]
            pair_part[piece] = sums[piece_rows:]

        @pl.when(jnp.logical_and(i >= 6, i < 6 + 2 * KEY_GROUPS))
        def _():
            block = i - 6

            @pl.when(lax.rem(block, 2) == 0)
            def _():
                for g in range(key_group):
                    share(block // 2 * key_group + g).wait_recv()

            for tile in range(tiles_count):
                attend_slice(tile, block)

        @pl.when(i >= 4)
        def _():
            m = i - 4
            piece = lax.rem(m + 2, pieces)
            part_copy(piece).wait_recv()

            @pl.when(m < 2)
            def _():
                total = own_part[piece].astype(F32) + pair_in[piece].astype(F32)
                leaving[m] = total.astype(BF16)

            @pl.when(m >= 2)
            def _():
                sum_copy(m - 2).wait_recv()
                total = own_part[piece].astype(F32) + pair_in[piece].astype(F32)
                total = (total + arrived[m - 2].astype(F32)).astype(BF16)

                @pl.when(m < pieces - 2)
                def _():
                    leaving[m] = total

                @pl.when(m >= pieces - 2)
                def _():
                    j = m - (pieces - 2)
                    main_back[j] = total[:held_main].reshape(main_back.shape[1:])
                    last_back[j] = total[held_main:]

            @pl.when(m < pieces - 2)
            def _():
                sum_copy(m).start()

        @pl.when(i == pieces)
        def _():
            for tile in range(tiles_count):
                mixed = row_acc[tile] / jnp.sum(row_sum[tile], axis=1, keepdims=True)
                mixed_send[tile * tile_groups : (tile + 1) * tile_groups] = mixed.astype(
                    BF16
                ).reshape(tile_groups, rows, LANES)

        return 0

    lax.fori_loop(0, pieces + 4, step, 0)
    for copy in row_copies + head_copies:
        copy.wait_send()

    tiles = jnp.zeros((last_rows, LANES), F32)
    for j in range(local_experts):
        for c in range(column_tiles):
            spot = place(last_rows, ep_count, j * column_tiles + c, local_experts * column_tiles)
            tiles = tiles + matmul(spot, last_back[j, :, c * LANES : (c + 1) * LANES])
    last_send[...] = tiles.astype(BF16).reshape(last_send.shape)
    back_copies = exchange_copies(
        "ep",
        (lambda e: main_back.at[:, e], lambda e: last_send.at[e]),
        (lambda e: main_recv.at[e], lambda e: last_recv.at[e]),
        (main_back_sems.at[0], last_back_sems.at[0]),
        (main_back_sems.at[1], last_back_sems.at[1]),
    )
    mixed_copies = exchange_copies(
        "tp",
        (lambda t: mixed_send.at[t],),
        (lambda t: mixed_recv.at[t],),
        (mixed_sems.at[0],),
        (mixed_sems.at[1],),
    )
    for copy in back_copies + mixed_copies:
        copy.start()
    mixed_recv[tp_me] = mixed_send[tp_me]
    last_recv[ep_me] = last_send[ep_me]
    for j in range(local_experts):
        main_recv[ep_me, j] = main_back[j, ep_me]

    def finish(i, _):
        @pl.when(i < pieces - 2)
        def _():
            ring_copy(i).wait_send()
            sum_copy(i).wait_send()

        pair_copy(i).wait_send()
        part_copy(i).wait_send()
        return 0

    lax.fori_loop(0, pieces, finish, 0)
    for copy in key_copies:
        copy.wait_send()

    def finish_share(d, _):
        share(d).wait_send()
        return 0

    lax.fori_loop(0, ep_count, finish_share, 0)

    main, last = slot_rows(ids_ref[...], experts, capacity)
    takers = []
    for k in range(len(main)):
        slot = jnp.where(main[k] >= 0, main[k], jnp.where(last[k] >= 0, last[k] + main_rows, -1))
        spot = (iota((results.shape[0], tokens), 0) == slot).astype(F32)
        takers.append(jnp.transpose(spot).astype(BF16))
    results[main_rows:, :] = jnp.zeros((results.shape[0] - main_rows, width), BF16)
    for copy in mixed_copies:
        copy.wait()
    heads = []
    for t in range(tp_count // 2):
        even, odd = mixed_recv[2 * t].astype(F32), mixed_recv[2 * t + 1].astype(F32)
        heads.append(jnp.where(lower, pltpu.roll(even, HEAD, 1), odd).astype(BF16))
    mix_out[...] = matmul(jnp.concatenate(heads, axis=1), w_out[...]).astype(BF16)

    for copy in back_copies:
        copy.wait()
    results[:main_rows, :] = main_recv[...].reshape(main_rows, width)
    tiles = last_recv[...].reshape(last_rows, LANES)
    for c in range(column_tiles):
        chosen = matmul(pick(experts, last_rows, c, column_tiles), tiles)
        results[main_rows : main_rows + experts, c * LANES : (c + 1) * LANES] = chosen.astype(BF16)
    combined = jnp.zeros((tokens, width), F32)
    for k, taker in enumerate(takers):
        row = jnp.broadcast_to(weights_ref[k : k + 1, :], (tokens, tokens))
        combined = combined + jnp.transpose(row)[:, :1] * matmul(taker, results[...])
    experts_out[...] = combined.astype(BF16)


def layer(
    mix, mix_gain, w_query, w_key, w_value, query_gain, key_gain, powers, w_out, tokens, gain, ids,
    weights, w_gate, w_up, w_down, capacity,
):
    pieces, ep_count = lax.axis_size("tp"), lax.axis_size("ep")
    rows, width = mix.shape
    local_experts = w_gate.shape[0]
    piece = (ep_count * capacity, width)
    head = pltpu.VMEM((pieces, rows, LANES), BF16)
    query_tile = math.gcd(pieces * rows, 256)
    state = pltpu.VMEM((pieces * rows // query_tile, query_tile, LANES), F32)
    by_device = pltpu.VMEM((ep_count, local_experts, capacity - 1, width), BF16)
    by_expert = pltpu.VMEM((local_experts, ep_count, capacity - 1, width), BF16)
    last = pltpu.VMEM((ep_count, local_experts * width // LANES, LANES), BF16)
    sums = pltpu.VMEM((pieces,) + piece, BF16)
    flights = pltpu.VMEM((pieces - 2,) + piece, BF16)
    result_rows = -(-local_experts * ep_count * capacity // LANES) * LANES
    return pl.pallas_call(
        layer_body,
        out_shape=[
            jax.ShapeDtypeStruct((rows, w_out.shape[1]), BF16),
            jax.ShapeDtypeStruct(tokens.shape, BF16),
        ],
        in_specs=[VMEM_SPEC] * 2
        + [HBM_SPEC] * 3
        + [VMEM_SPEC] * 3
        + [HBM_SPEC]
        + [VMEM_SPEC] * 4
        + [HBM_SPEC] * 3,
        out_specs=[VMEM_SPEC] * 2,
        scratch_shapes=[
            pltpu.VMEM(w.shape, BF16) for w in (w_query, w_key, w_value, w_out, w_gate, w_up, w_down)
        ]
        + [head, head, by_device, by_expert, last, last]
        + [pltpu.VMEM((pieces, 2) + piece, BF16), sums, sums, sums, flights, flights]
        + [pltpu.VMEM((2, ep_count, pieces, rows // 2, LANES), BF16), head, state, state, state]
        + [head, head, by_expert, by_device]
        + [pltpu.VMEM((local_experts, ep_count, width), BF16), last]
        + [pltpu.VMEM((result_rows, width), BF16)]
        + [DMA((7,)), DMA((2, pieces)), DMA((2, ep_count)), DMA((2, ep_count))]
        + [DMA((2, pieces))] * 4
        + [DMA((2, ep_count))] * 2
        + [DMA((2, pieces)), DMA((2, ep_count)), DMA((2, ep_count))],
        name="layer",
        compiler_params=pltpu.CompilerParams(
            collective_id=0, has_side_effects=True, vmem_limit_bytes=62 * MIB
        ),
    )(
        mix, mix_gain, w_query, w_key, w_value, query_gain, key_gain, powers, w_out, tokens, gain,
        ids, weights, w_gate, w_up, w_down,
    )


def body(
    mix_tokens,
    mix_gain,
    w_query,
    w_key,
    w_value,
    query_gain,
    key_gain,
    w_out,
    expert_tokens,
    expert_gain,
    route_ids,
    route_weights,
    w_gate,
    w_up,
    w_down,
):
    ep_count = lax.axis_size("ep")
    seq_rows, _, model_width = mix_tokens.shape
    tok_count, top_count = route_ids.shape
    local_experts = w_gate.shape[0]
    capacity = tok_count * top_count * 9 // (8 * local_experts * ep_count)
    id_rows = jnp.transpose(route_ids)
    mix_out, experts_out = layer(
        mix_tokens.reshape(seq_rows, model_width),
        mix_gain.reshape(1, model_width),
        w_query,
        w_key,
        w_value,
        query_gain.reshape(1, HEAD),
        key_gain.reshape(1, HEAD),
        frequencies(),
        w_out,
        expert_tokens,
        expert_gain.reshape(1, model_width),
        id_rows,
        jnp.transpose(route_weights),
        w_gate,
        w_up,
        w_down,
        capacity,
    )
    return (mix_out[:, None, :], experts_out)


def solution(mesh):
    placed = (
        P(("ep", "tp"), None, None),
        P(),
        P(),
        P(),
        P(),
        P(),
        P(),
        P(),
        P(("ep", "tp"), None),
        P(),
        P(("ep", "tp"), None),
        P(("ep", "tp"), None),
        P("ep", None, "tp"),
        P("ep", None, "tp"),
        P("ep", "tp", None),
    )
    return jax.shard_map(
        body,
        mesh=mesh,
        in_specs=placed,
        out_specs=(P(("ep", "tp"), None, None), P(("ep", "tp"), None)),
        check_vma=False,
    )
```

```python
import functools
import math

import jax
import jax.numpy as jnp
from jax import lax
from jax.experimental import pallas as pl
from jax.experimental.pallas import tpu as pltpu
import numpy as np
from jax.sharding import PartitionSpec as P

HEAD = 64
GRID_W = 64
LANES = 128
KEY_GROUPS = 4
EXP2_SCALE = HEAD ** (-0.5) * math.log2(math.e)
MESH = pl.DeviceIdType.MESH
MIB = 1024 * 1024
BF16, F32 = jnp.bfloat16, jnp.float32
VMEM_SPEC = pl.BlockSpec(memory_space=pltpu.VMEM)
HBM_SPEC = pl.BlockSpec(memory_space=pltpu.HBM)
DMA = pltpu.SemaphoreType.DMA


epsilon = 1e-06


def normalize(values, gain_vec):
    widened = values.astype(F32)
    return (
        widened
        * lax.rsqrt(jnp.mean(widened * widened, axis=-1, keepdims=True) + epsilon)
        * gain_vec
    )


def matmul(left, right):
    return jnp.dot(left, right, preferred_element_type=F32)


def frequencies():
    quarter = HEAD // 4
    powers = np.float32(10000.0) ** (-np.arange(quarter, dtype=np.float32) / np.float32(quarter))
    return np.tile(powers.astype(np.float32), LANES // quarter).reshape(1, LANES)


def greet(peers):
    barrier = pltpu.get_barrier_semaphore()
    for peer in peers:
        pl.semaphore_signal(barrier, inc=1, device_id=peer, device_id_type=MESH)


def await_greetings(count):
    pl.semaphore_wait(pltpu.get_barrier_semaphore(), count)


def axis_peers(axis):
    me, count = lax.axis_index(axis), lax.axis_size(axis)
    return [lax.rem(me + d, count) for d in range(count)]


def remote(source, target, send_sem, recv_sem, device_id):
    return pltpu.make_async_remote_copy(
        src_ref=source,
        dst_ref=target,
        send_sem=send_sem,
        recv_sem=recv_sem,
        device_id=device_id,
        device_id_type=MESH,
    )


def exchange_copies(axis, sources, targets, sends, recvs):
    me = lax.axis_index(axis)
    return [
        remote(source(peer), target(me), send.at[d], recv.at[d], {axis: peer})
        for d, peer in enumerate(axis_peers(axis))
        if d > 0
        for source, target, send, recv in zip(sources, targets, sends, recvs)
    ]


def iota(shape, axis):
    return lax.broadcasted_iota(jnp.int32, shape, axis)


def slot_rows(id_rows, experts, capacity):
    choices, tokens = id_rows.shape
    marks = [
        (iota((experts, tokens), 0) == id_rows[k : k + 1, :]).astype(F32) for k in range(choices)
    ]
    earlier = (iota((tokens, tokens), 0) < iota((tokens, tokens), 1)).astype(BF16)
    ranks = matmul(functools.reduce(jnp.add, marks).astype(BF16), earlier)
    main, last = [], []
    for k in range(choices):
        rank = jnp.sum(marks[k] * ranks, axis=0, keepdims=True).astype(jnp.int32)
        ids = id_rows[k : k + 1, :]
        main.append(jnp.where(rank < capacity - 1, ids * (capacity - 1) + rank, -1))
        last.append(jnp.where(rank == capacity - 1, ids, -1))
    return main, last


def pick(rows, columns, first, stride):
    wanted = iota((rows, columns), 0) * stride + first
    return (iota((rows, columns), 1) == wanted).astype(BF16)


def place(rows, columns, first, stride):
    wanted = iota((rows, columns), 1) * stride + first
    return (iota((rows, columns), 0) == wanted).astype(BF16)


def head_turner(first, rows, powers, pair_sums):
    lane = iota((rows, LANES), 1)
    quarter = HEAD // 4
    position = first + iota((rows, LANES), 0)
    by_row = lax.rem(lane, HEAD) < HEAD // 2
    place = jnp.where(by_row, position // GRID_W, lax.rem(position, GRID_W)).astype(F32)
    angles = place * powers
    cosine = jnp.cos(angles)
    sine = jnp.sin(angles)
    sine = jnp.where(lax.rem(lane, 2 * quarter) < quarter, -sine, sine)

    def turned(raw, gain):
        values = raw.astype(BF16).astype(F32)
        squares = values * values
        high = squares.astype(BF16)
        low = (squares - high.astype(F32)).astype(BF16)
        sums = matmul(high, pair_sums) + matmul(low, pair_sums)
        values = values * lax.rsqrt(sums * (1.0 / HEAD) + epsilon) * gain
        partner = jnp.where(
            lax.rem(lane, 2 * quarter) < quarter,
            pltpu.roll(values, LANES - quarter, 1),
            pltpu.roll(values, quarter, 1),
        )
        return (values * cosine + partner * sine).astype(BF16).astype(F32)

    return turned


def ring_places():
    me = lax.axis_index("tp")
    chips = lax.axis_size("tp") // 2
    chip, core = me // 2, lax.rem(me, 2)
    ahead = lax.rem(chip + 1 - 2 * core + chips, chips) * 2 + core
    behind = lax.rem(chip - 1 + 2 * core + chips, chips) * 2 + core
    partner = chip * 2 + 1 - core
    return core, {"tp": ahead}, {"tp": behind}, {"tp": partner}


def layer_body(
    mix_ref,
    mix_gain_ref,
    query_hbm,
    key_hbm,
    value_hbm,
    query_gain_ref,
    key_gain_ref,
    powers_ref,
    out_hbm,
    token_ref,
    token_gain_ref,
    ids_ref,
    weights_ref,
    gate_hbm,
    up_hbm,
    down_hbm,
    mix_out,
    experts_out,
    w_query,
    w_key,
    w_value,
    w_out,
    gate,
    up,
    down,
    head_send,
    head_recv,
    rows_send,
    rows_in,
    held,
    own_part,
    pair_part,
    pair_in,
    leaving,
    arrived,
    keys,
    queries,
    row_max,
    row_sum,
    row_acc,
    mixed_send,
    mixed_recv,
    rows_back,
    rows_recv,
    results,
    load_sem,
    head_sems,
    row_sems,
    ring_sems,
    pair_sems,
    part_sems,
    sum_sems,
    key_sems,
    share_sems,
    mixed_sems,
    back_sems,
):
    tp_count, ep_count = lax.axis_size("tp"), lax.axis_size("ep")
    tp_me, ep_me = lax.axis_index("tp"), lax.axis_index("ep")
    core, ahead, behind, partner = ring_places()
    greet([{"tp": p} for p in axis_peers("tp")[1:]] + [{"ep": p} for p in axis_peers("ep")[1:]])
    loads = [
        pltpu.make_async_copy(hbm, vmem, load_sem.at[i])
        for i, (hbm, vmem) in enumerate(
            (
                (query_hbm, w_query),
                (key_hbm, w_key),
                (value_hbm, w_value),
                (gate_hbm, gate),
                (up_hbm, up),
                (down_hbm, down),
                (out_hbm, w_out),
            )
        )
    ]
    for load in loads:
        load.start()

    _, local_experts, _, main_cap, _ = rows_send.shape
    width = token_ref.shape[1]
    column_tiles = width // LANES
    tile_shape = (ep_count, local_experts, main_cap, LANES)
    experts = local_experts * ep_count
    capacity = main_cap + 1
    tokens = token_ref.shape[0]
    main_rows, last_rows = experts * main_cap, experts * column_tiles
    normed = normalize(token_ref[...], token_gain_ref[...]).astype(BF16)
    main, last = slot_rows(ids_ref[...], experts, capacity)
    slots = iota((main_rows, tokens), 0)
    hits = functools.reduce(jnp.add, [(slots == row).astype(F32) for row in main])
    outgoing = matmul(hits.astype(BF16), normed).astype(BF16)
    for c in range(column_tiles):
        rows_send[:, :, c] = outgoing[:, c * LANES : (c + 1) * LANES].reshape(tile_shape)
    slots = iota((last_rows, tokens), 0)
    tiles = jnp.zeros((last_rows, LANES), F32)
    for c in range(column_tiles):
        hits = [
            (slots == jnp.where(row >= 0, row * column_tiles + c, -1)).astype(F32) for row in last
        ]
        hits = functools.reduce(jnp.add, hits).astype(BF16)
        tiles = tiles + matmul(hits, normed[:, c * LANES : (c + 1) * LANES])
    rows_send[:, :, column_tiles] = tiles.astype(BF16).reshape(tile_shape)
    await_greetings(tp_count + ep_count - 2)
    row_copies = [
        exchange_copies(
            "ep",
            (lambda e, j=j: rows_send.at[e, j],),
            (lambda e, j=j: rows_in.at[e, j],),
            (row_sems.at[0, j],),
            (row_sems.at[1, j],),
        )
        for j in range(local_experts)
    ]
    for copy in row_copies[0] + row_copies[1]:
        copy.start()

    normed = normalize(mix_ref[...], mix_gain_ref[...]).astype(BF16)
    rows = normed.shape[0]
    half = rows // 2
    pair_sums = iota((LANES, LANES), 0) // HEAD == iota((LANES, LANES), 1) // HEAD
    turned = head_turner(
        (ep_me * tp_count + tp_me) * rows, rows, powers_ref[...], pair_sums.astype(BF16)
    )
    query_gain = jnp.concatenate([query_gain_ref[...]] * (LANES // HEAD), axis=1)
    key_gain = jnp.concatenate([key_gain_ref[...]] * (LANES // HEAD), axis=1)
    lower = iota((rows, LANES), 1) < HEAD
    lower_half = iota((half, LANES), 1) < HEAD
    for load in loads[:3]:
        load.wait()
    raw_keys, raw_values = matmul(normed, w_key[...]), matmul(normed, w_value[...])
    key_heads = w_key.shape[1] // HEAD
    group = tp_count // key_heads
    for t in range(key_heads // 2):
        key = turned(raw_keys[:, t * LANES : (t + 1) * LANES], key_gain)
        value = raw_values[:, t * LANES : (t + 1) * LANES].astype(BF16).astype(F32)
        for h, pairs in enumerate(
            (
                jnp.where(lower, key, pltpu.roll(value, HEAD, 1)),
                jnp.where(lower, pltpu.roll(key, HEAD, 1), value),
            )
        ):
            pairs = pairs.astype(BF16)
            for member in range(group):
                part = member % 2 * half
                head_send[(2 * t + h) * group + member, :half, :] = pairs[part : part + half]
    raw_queries = matmul(normed, w_query[...])
    for t in range(tp_count // 2):
        tile = turned(raw_queries[:, t * LANES : (t + 1) * LANES], query_gain)
        first, second = tile[:half], tile[half:]
        head_send[2 * t, half:, :] = jnp.where(
            lower_half, first, pltpu.roll(second, HEAD, 1)
        ).astype(BF16)
        head_send[2 * t + 1, half:, :] = jnp.where(
            lower_half, pltpu.roll(first, HEAD, 1), second
        ).astype(BF16)
    head_copies = exchange_copies(
        "tp",
        (lambda t: head_send.at[t],),
        (lambda t: head_recv.at[t],),
        (head_sems.at[0],),
        (head_sems.at[1],),
    )
    for copy in head_copies:
        copy.start()
    head_recv[tp_me] = head_send[tp_me]
    rows_in[ep_me] = rows_send[ep_me]
    row_max[...] = jnp.full(row_max.shape, -1e30, F32)
    row_sum[...] = jnp.zeros(row_sum.shape, F32)
    row_acc[...] = jnp.zeros(row_acc.shape, F32)

    pieces, _, piece_rows, _ = held.shape
    held_main = ep_count * main_cap

    def receive_rows(j):
        for copy in row_copies[j]:
            copy.wait_recv()
        tiles = rows_in[:, j, column_tiles].reshape(ep_count * column_tiles, LANES)
        for c in range(column_tiles):
            columns = slice(c * LANES, (c + 1) * LANES)
            chosen = matmul(pick(ep_count, ep_count * column_tiles, c, column_tiles), tiles)
            held[j, 0, :held_main, columns] = rows_in[:, j, c].reshape(held_main, LANES)
            held[j, 0, held_main:, columns] = chosen.astype(BF16)

    def ring_copy(i):
        return remote(
            held.at[i, 0], held.at[i + 2, 0], ring_sems.at[0, i], ring_sems.at[1, i], ahead
        )

    def pair_copy(i):
        return remote(
            held.at[i, 0], held.at[i, 1], pair_sems.at[0, i], pair_sems.at[1, i], partner
        )

    def part_copy(i):
        return remote(
            pair_part.at[i], pair_in.at[i], part_sems.at[0, i], part_sems.at[1, i], partner
        )

    def sum_copy(m):
        return remote(leaving.at[m], arrived.at[m], sum_sems.at[0, m], sum_sems.at[1, m], ahead)

    own_keys = head_recv.at[:, pl.ds(0, half), :]
    key_copies = [
        remote(
            own_keys, keys.at[core, d], key_sems.at[0, d], key_sems.at[1, d], {"ep": peer}
        )
        for d, peer in enumerate(axis_peers("ep"))
        if d > 0
    ]

    def key_arrival(d):
        return remote(
            keys.at[core, d], keys.at[core, d], key_sems.at[0, d], key_sems.at[1, d], partner
        )

    def share(d):
        return remote(
            keys.at[core, d], keys.at[core, d], share_sems.at[0, d], share_sems.at[1, d], partner
        )

    tiles_count, tile_rows, _ = row_acc.shape
    tile_groups = tile_rows // rows
    groups = tp_count
    key_group = ep_count // KEY_GROUPS
    key_rows = key_group * groups * half

    def attend_slice(tile, block):
        chosen = queries[tile * tile_groups : (tile + 1) * tile_groups].reshape(tile_rows, LANES)
        pairs = keys[lax.rem(block, 2), pl.ds(block // 2 * key_group, key_group)]
        pairs = pairs.reshape(key_rows, LANES)
        scores = lax.dot_general(
            chosen, pairs, (((1,), (1,)), ((), ())), preferred_element_type=F32
        )
        old_max = row_max[tile][:, :1]
        new_max = jnp.maximum(old_max, jnp.max(scores, axis=1, keepdims=True))
        shrink = jnp.exp2((old_max - new_max) * EXP2_SCALE)
        raised = jnp.exp2((scores - new_max) * EXP2_SCALE)
        lane_sums = raised[:, :LANES]
        for lane in range(LANES, key_rows, LANES):
            lane_sums = lane_sums + raised[:, lane : lane + LANES]
        row_max[tile] = jnp.broadcast_to(new_max, (tile_rows, LANES))
        row_sum[tile] = row_sum[tile] * shrink + lane_sums
        row_acc[tile] = row_acc[tile] * shrink + matmul(raised.astype(BF16), pairs)

    back_copies = [
        exchange_copies(
            "ep",
            (lambda e, j=j: rows_back.at[e, j],),
            (lambda e, j=j: rows_recv.at[e, j],),
            (back_sems.at[0, j],),
            (back_sems.at[1, j],),
        )
        for j in range(local_experts)
    ]
    mixed_copies = exchange_copies(
        "tp",
        (lambda t: mixed_send.at[t],),
        (lambda t: mixed_recv.at[t],),
        (mixed_sems.at[0],),
        (mixed_sems.at[1],),
    )

    def return_rows(j, total):
        tiles = jnp.zeros((ep_count * column_tiles, LANES), F32)
        for c in range(column_tiles):
            columns = slice(c * LANES, (c + 1) * LANES)
            rows_back[:, j, c] = total[:held_main, columns].reshape(ep_count, main_cap, LANES)
            spot = place(ep_count * column_tiles, ep_count, c, column_tiles)
            tiles = tiles + matmul(spot, total[held_main:, columns])
        tiles = tiles.astype(BF16).reshape(ep_count, main_cap, LANES)
        rows_back[:, j, column_tiles] = tiles
        for copy in back_copies[j]:
            copy.start()

    def step(i, _):
        @pl.when(jnp.logical_and(i >= 2, i < pieces + 2))
        def _():
            part_copy(i - 2).start()

        for j in range(local_experts):

            @pl.when(i == j)
            def _(j=j):
                receive_rows(j)

        @pl.when(i < pieces)
        def _():
            @pl.when(i >= 2)
            def _():
                ring_copy(i - 2).wait_recv()

            @pl.when(i < pieces - 2)
            def _():
                ring_copy(i).start()

            pair_copy(i).start()

        @pl.when(i == 1)
        def _():
            for load in loads[3:]:
                load.wait()

        @pl.when(i == 2)
        def _():
            for copy in head_copies:
                copy.wait_recv()
            for copy in key_copies:
                copy.start()
            keys[core, 0] = head_recv[:, :half, :]
            packed = head_recv[:, half:, :].astype(F32).reshape(groups * half, LANES)
            lower_lanes = iota(packed.shape, 1) < HEAD
            for h, values in enumerate((packed, pltpu.roll(packed, HEAD, 1))):
                values = jnp.where(lower_lanes, values, 0.0).astype(BF16)
                queries[:, h * half : (h + 1) * half, :] = values.reshape(groups, half, LANES)

        @pl.when((i >= 5) & (i < 5 + 2 * KEY_GROUPS) & (lax.rem(i, 2) == 1))
        def _():
            for g in range(key_group):
                d = (i - 5) // 2 * key_group + g

                @pl.when(d > 0)
                def _():
                    key_arrival(d).wait_recv()

                share(d).start()

        @pl.when(jnp.logical_and(i >= 1, i <= pieces))
        def _():
            piece = i - 1
            expert = lax.rem(piece, 2)
            pair_copy(piece).wait_recv()
            values = held[piece].reshape(2 * piece_rows, width)
            gate_act = matmul(values, gate[expert])
            up_act = matmul(values, up[expert])
            hidden = (gate_act / (1.0 + jnp.exp(-gate_act)) * up_act).astype(BF16)
            sums = matmul(hidden, down[expert]).astype(BF16)
            own_part[piece] = sums[:piece_rows]
            pair_part[piece] = sums[piece_rows:]

        @pl.when(jnp.logical_and(i >= 7, i < 7 + 2 * KEY_GROUPS))
        def _():
            block = i - 7

            @pl.when(lax.rem(block, 2) == 0)
            def _():
                for g in range(key_group):
                    share(block // 2 * key_group + g).wait_recv()

            for tile in range(tiles_count):
                attend_slice(tile, block)

        @pl.when(i >= 4)
        def _():
            m = i - 4
            piece = lax.rem(m + 2, pieces)
            part_copy(piece).wait_recv()

            @pl.when(m < 2)
            def _():
                total = own_part[piece].astype(F32) + pair_in[piece].astype(F32)
                leaving[m] = total.astype(BF16)

            @pl.when(m >= 2)
            def _():
                sum_copy(m - 2).wait_recv()
                total = own_part[piece].astype(F32) + pair_in[piece].astype(F32)
                total = (total + arrived[m - 2].astype(F32)).astype(BF16)

                @pl.when(m < pieces - 2)
                def _():
                    leaving[m] = total

                for j in range(local_experts):

                    @pl.when(m == pieces - 2 + j)
                    def _(j=j):
                        return_rows(j, total)

            @pl.when(m < pieces - 2)
            def _():
                sum_copy(m).start()

        @pl.when(i == pieces)
        def _():
            for tile in range(tiles_count):
                mixed = row_acc[tile] / jnp.sum(row_sum[tile], axis=1, keepdims=True)
                mixed_send[tile * tile_groups : (tile + 1) * tile_groups] = mixed.astype(
                    BF16
                ).reshape(tile_groups, rows, LANES)

        return 0

    lax.fori_loop(0, pieces + 4, step, 0)
    for copy in mixed_copies:
        copy.start()
    mixed_recv[tp_me] = mixed_send[tp_me]
    rows_recv[ep_me] = rows_back[ep_me]
    for copy in row_copies[0] + row_copies[1] + head_copies:
        copy.wait_send()

    def finish(i, _):
        @pl.when(i < pieces - 2)
        def _():
            ring_copy(i).wait_send()
            sum_copy(i).wait_send()

        pair_copy(i).wait_send()
        part_copy(i).wait_send()
        return 0

    lax.fori_loop(0, pieces, finish, 0)
    for copy in key_copies:
        copy.wait_send()

    def finish_share(d, _):
        share(d).wait_send()
        return 0

    lax.fori_loop(0, ep_count, finish_share, 0)

    main, last = slot_rows(ids_ref[...], experts, capacity)
    takers = []
    for k in range(len(main)):
        slot = jnp.where(main[k] >= 0, main[k], jnp.where(last[k] >= 0, last[k] + main_rows, -1))
        spot = (iota((results.shape[0], tokens), 0) == slot).astype(F32)
        takers.append(jnp.transpose(spot).astype(BF16))
    results[main_rows:, :] = jnp.zeros((results.shape[0] - main_rows, width), BF16)
    for copy in mixed_copies:
        copy.wait()
    heads = []
    for t in range(tp_count // 2):
        even, odd = mixed_recv[2 * t].astype(F32), mixed_recv[2 * t + 1].astype(F32)
        heads.append(jnp.where(lower, pltpu.roll(even, HEAD, 1), odd).astype(BF16))
    mix_out[...] = matmul(jnp.concatenate(heads, axis=1), w_out[...]).astype(BF16)

    for copy in back_copies[0] + back_copies[1]:
        copy.wait()
    tiles = rows_recv[:, :, column_tiles].reshape(last_rows, LANES)
    for c in range(column_tiles):
        columns = slice(c * LANES, (c + 1) * LANES)
        results[:main_rows, columns] = rows_recv[:, :, c].reshape(main_rows, LANES)
        chosen = matmul(pick(experts, last_rows, c, column_tiles), tiles)
        results[main_rows : main_rows + experts, columns] = chosen.astype(BF16)
    combined = jnp.zeros((tokens, width), F32)
    for k, taker in enumerate(takers):
        row = jnp.broadcast_to(weights_ref[k : k + 1, :], (tokens, tokens))
        combined = combined + jnp.transpose(row)[:, :1] * matmul(taker, results[...])
    experts_out[...] = combined.astype(BF16)


def layer(
    mix, mix_gain, w_query, w_key, w_value, query_gain, key_gain, powers, w_out, tokens, gain, ids,
    weights, w_gate, w_up, w_down, capacity,
):
    pieces, ep_count = lax.axis_size("tp"), lax.axis_size("ep")
    rows, width = mix.shape
    local_experts = w_gate.shape[0]
    piece = (ep_count * capacity, width)
    head = pltpu.VMEM((pieces, rows, LANES), BF16)
    query_tile = math.gcd(pieces * rows, 256)
    state = pltpu.VMEM((pieces * rows // query_tile, query_tile, LANES), F32)
    column_tiles = width // LANES
    assert column_tiles == capacity - 1
    block = pltpu.VMEM((ep_count, local_experts, column_tiles + 1, capacity - 1, LANES), BF16)
    sums = pltpu.VMEM((pieces,) + piece, BF16)
    flights = pltpu.VMEM((pieces - 2,) + piece, BF16)
    result_rows = -(-local_experts * ep_count * capacity // LANES) * LANES
    return pl.pallas_call(
        layer_body,
        out_shape=[
            jax.ShapeDtypeStruct((rows, w_out.shape[1]), BF16),
            jax.ShapeDtypeStruct(tokens.shape, BF16),
        ],
        in_specs=[VMEM_SPEC] * 2
        + [HBM_SPEC] * 3
        + [VMEM_SPEC] * 3
        + [HBM_SPEC]
        + [VMEM_SPEC] * 4
        + [HBM_SPEC] * 3,
        out_specs=[VMEM_SPEC] * 2,
        scratch_shapes=[
            pltpu.VMEM(w.shape, BF16) for w in (w_query, w_key, w_value, w_out, w_gate, w_up, w_down)
        ]
        + [head, head, block, block]
        + [pltpu.VMEM((pieces, 2) + piece, BF16), sums, sums, sums, flights, flights]
        + [pltpu.VMEM((2, ep_count, pieces, rows // 2, LANES), BF16), head, state, state, state]
        + [head, head, block, block]
        + [pltpu.VMEM((result_rows, width), BF16)]
        + [DMA((7,)), DMA((2, pieces)), DMA((2, local_experts, ep_count))]
        + [DMA((2, pieces))] * 4
        + [DMA((2, ep_count))] * 2
        + [DMA((2, pieces)), DMA((2, local_experts, ep_count))],
        name="layer",
        compiler_params=pltpu.CompilerParams(
            collective_id=0, has_side_effects=True, vmem_limit_bytes=62 * MIB
        ),
    )(
        mix, mix_gain, w_query, w_key, w_value, query_gain, key_gain, powers, w_out, tokens, gain,
        ids, weights, w_gate, w_up, w_down,
    )


def body(
    mix_tokens,
    mix_gain,
    w_query,
    w_key,
    w_value,
    query_gain,
    key_gain,
    w_out,
    expert_tokens,
    expert_gain,
    route_ids,
    route_weights,
    w_gate,
    w_up,
    w_down,
):
    ep_count = lax.axis_size("ep")
    seq_rows, _, model_width = mix_tokens.shape
    tok_count, top_count = route_ids.shape
    local_experts = w_gate.shape[0]
    capacity = tok_count * top_count * 9 // (8 * local_experts * ep_count)
    id_rows = jnp.transpose(route_ids)
    mix_out, experts_out = layer(
        mix_tokens.reshape(seq_rows, model_width),
        mix_gain.reshape(1, model_width),
        w_query,
        w_key,
        w_value,
        query_gain.reshape(1, HEAD),
        key_gain.reshape(1, HEAD),
        frequencies(),
        w_out,
        expert_tokens,
        expert_gain.reshape(1, model_width),
        id_rows,
        jnp.transpose(route_weights),
        w_gate,
        w_up,
        w_down,
        capacity,
    )
    return (mix_out[:, None, :], experts_out)


def solution(mesh):
    placed = (
        P(("ep", "tp"), None, None),
        P(),
        P(),
        P(),
        P(),
        P(),
        P(),
        P(),
        P(("ep", "tp"), None),
        P(),
        P(("ep", "tp"), None),
        P(("ep", "tp"), None),
        P("ep", None, "tp"),
        P("ep", None, "tp"),
        P("ep", "tp", None),
    )
    return jax.shard_map(
        body,
        mesh=mesh,
        in_specs=placed,
        out_specs=(P(("ep", "tp"), None, None), P(("ep", "tp"), None)),
        check_vma=False,
    )
```

```python
import functools
import math

import jax
import jax.numpy as jnp
from jax import lax
from jax.experimental import pallas as pl
from jax.experimental.pallas import tpu as pltpu
import numpy as np
from jax.sharding import PartitionSpec as P

HEAD = 64
GRID_W = 64
LANES = 128
KEY_GROUPS = 4
EXP2_SCALE = HEAD ** (-0.5) * math.log2(math.e)
MESH = pl.DeviceIdType.MESH
MIB = 1024 * 1024
BF16, F32 = jnp.bfloat16, jnp.float32
VMEM_SPEC = pl.BlockSpec(memory_space=pltpu.VMEM)
HBM_SPEC = pl.BlockSpec(memory_space=pltpu.HBM)
DMA = pltpu.SemaphoreType.DMA


epsilon = 1e-06


def normalize(values, gain_vec):
    widened = values.astype(F32)
    return (
        widened
        * lax.rsqrt(jnp.mean(widened * widened, axis=-1, keepdims=True) + epsilon)
        * gain_vec
    )


def matmul(left, right):
    return jnp.dot(left, right, preferred_element_type=F32)


def frequencies():
    quarter = HEAD // 4
    powers = np.float32(10000.0) ** (-np.arange(quarter, dtype=np.float32) / np.float32(quarter))
    return np.tile(powers.astype(np.float32), LANES // quarter).reshape(1, LANES)


def greet(peers):
    barrier = pltpu.get_barrier_semaphore()
    for peer in peers:
        pl.semaphore_signal(barrier, inc=1, device_id=peer, device_id_type=MESH)


def await_greetings(count):
    pl.semaphore_wait(pltpu.get_barrier_semaphore(), count)


def axis_peers(axis):
    me, count = lax.axis_index(axis), lax.axis_size(axis)
    return [lax.rem(me + d, count) for d in range(count)]


def remote(source, target, send_sem, recv_sem, device_id):
    return pltpu.make_async_remote_copy(
        src_ref=source,
        dst_ref=target,
        send_sem=send_sem,
        recv_sem=recv_sem,
        device_id=device_id,
        device_id_type=MESH,
    )


def exchange_copies(axis, sources, targets, sends, recvs):
    me = lax.axis_index(axis)
    return [
        remote(source(peer), target(me), send.at[d], recv.at[d], {axis: peer})
        for d, peer in enumerate(axis_peers(axis))
        if d > 0
        for source, target, send, recv in zip(sources, targets, sends, recvs)
    ]


def iota(shape, axis):
    return lax.broadcasted_iota(jnp.int32, shape, axis)


def slot_rows(id_rows, experts, capacity):
    choices, tokens = id_rows.shape
    marks = [
        (iota((experts, tokens), 0) == id_rows[k : k + 1, :]).astype(F32) for k in range(choices)
    ]
    earlier = (iota((tokens, tokens), 0) < iota((tokens, tokens), 1)).astype(BF16)
    ranks = matmul(functools.reduce(jnp.add, marks).astype(BF16), earlier)
    main, last = [], []
    for k in range(choices):
        rank = jnp.sum(marks[k] * ranks, axis=0, keepdims=True).astype(jnp.int32)
        ids = id_rows[k : k + 1, :]
        main.append(jnp.where(rank < capacity - 1, ids * (capacity - 1) + rank, -1))
        last.append(jnp.where(rank == capacity - 1, ids, -1))
    return main, last


def pick(rows, columns, first, stride):
    wanted = iota((rows, columns), 0) * stride + first
    return (iota((rows, columns), 1) == wanted).astype(BF16)


def place(rows, columns, first, stride):
    wanted = iota((rows, columns), 1) * stride + first
    return (iota((rows, columns), 0) == wanted).astype(BF16)


def head_turner(first, rows, powers, pair_sums):
    lane = iota((rows, LANES), 1)
    quarter = HEAD // 4
    position = first + iota((rows, LANES), 0)
    by_row = lax.rem(lane, HEAD) < HEAD // 2
    place = jnp.where(by_row, position // GRID_W, lax.rem(position, GRID_W)).astype(F32)
    angles = place * powers
    cosine = jnp.cos(angles)
    sine = jnp.sin(angles)
    sine = jnp.where(lax.rem(lane, 2 * quarter) < quarter, -sine, sine)

    def turned(raw, gain):
        values = raw.astype(BF16).astype(F32)
        squares = values * values
        high = squares.astype(BF16)
        low = (squares - high.astype(F32)).astype(BF16)
        sums = matmul(high, pair_sums) + matmul(low, pair_sums)
        values = values * lax.rsqrt(sums * (1.0 / HEAD) + epsilon) * gain
        partner = jnp.where(
            lax.rem(lane, 2 * quarter) < quarter,
            pltpu.roll(values, LANES - quarter, 1),
            pltpu.roll(values, quarter, 1),
        )
        return (values * cosine + partner * sine).astype(BF16).astype(F32)

    return turned


def ring_places():
    me = lax.axis_index("tp")
    chips = lax.axis_size("tp") // 2
    chip, core = me // 2, lax.rem(me, 2)
    ahead = lax.rem(chip + 1 - 2 * core + chips, chips) * 2 + core
    behind = lax.rem(chip - 1 + 2 * core + chips, chips) * 2 + core
    partner = chip * 2 + 1 - core
    return core, {"tp": ahead}, {"tp": behind}, {"tp": partner}


def layer_body(
    mix_ref,
    mix_gain_ref,
    query_hbm,
    key_hbm,
    value_hbm,
    query_gain_ref,
    key_gain_ref,
    powers_ref,
    out_hbm,
    token_ref,
    token_gain_ref,
    ids_ref,
    weights_ref,
    gate_hbm,
    up_hbm,
    down_hbm,
    mix_out,
    experts_out,
    w_query,
    w_key,
    w_value,
    w_out,
    gate,
    up,
    down,
    head_send,
    head_recv,
    rows_send,
    rows_in,
    held,
    own_part,
    pair_part,
    pair_in,
    leaving,
    arrived,
    keys,
    queries,
    row_max,
    row_sum,
    row_acc,
    mixed_send,
    mixed_recv,
    rows_back,
    rows_recv,
    results,
    load_sem,
    head_sems,
    row_sems,
    ring_sems,
    pair_sems,
    part_sems,
    sum_sems,
    key_sems,
    share_sems,
    mixed_sems,
    back_sems,
):
    tp_count, ep_count = lax.axis_size("tp"), lax.axis_size("ep")
    tp_me, ep_me = lax.axis_index("tp"), lax.axis_index("ep")
    core, ahead, behind, partner = ring_places()
    greet([{"tp": p} for p in axis_peers("tp")[1:]] + [{"ep": p} for p in axis_peers("ep")[1:]])
    loads = [
        pltpu.make_async_copy(hbm, vmem, load_sem.at[i])
        for i, (hbm, vmem) in enumerate(
            (
                (query_hbm, w_query),
                (key_hbm, w_key),
                (value_hbm, w_value),
                (gate_hbm, gate),
                (up_hbm, up),
                (down_hbm, down),
                (out_hbm, w_out),
            )
        )
    ]
    for load in loads:
        load.start()

    _, local_experts, _, main_cap, _ = rows_send.shape
    width = token_ref.shape[1]
    column_tiles = width // LANES
    tile_shape = (ep_count, local_experts, main_cap, LANES)
    experts = local_experts * ep_count
    capacity = main_cap + 1
    tokens = token_ref.shape[0]
    main_rows, last_rows = experts * main_cap, experts * column_tiles
    normed = normalize(token_ref[...], token_gain_ref[...]).astype(BF16)
    main, last = slot_rows(ids_ref[...], experts, capacity)
    slots = iota((main_rows, tokens), 0)
    hits = functools.reduce(jnp.add, [(slots == row).astype(F32) for row in main])
    outgoing = matmul(hits.astype(BF16), normed).astype(BF16)
    for c in range(column_tiles):
        rows_send[:, :, c] = outgoing[:, c * LANES : (c + 1) * LANES].reshape(tile_shape)
    slots = iota((last_rows, tokens), 0)
    tiles = jnp.zeros((last_rows, LANES), F32)
    for c in range(column_tiles):
        hits = [
            (slots == jnp.where(row >= 0, row * column_tiles + c, -1)).astype(F32) for row in last
        ]
        hits = functools.reduce(jnp.add, hits).astype(BF16)
        tiles = tiles + matmul(hits, normed[:, c * LANES : (c + 1) * LANES])
    rows_send[:, :, column_tiles] = tiles.astype(BF16).reshape(tile_shape)
    await_greetings(tp_count + ep_count - 2)
    row_copies = [
        exchange_copies(
            "ep",
            (lambda e, j=j: rows_send.at[e, j],),
            (lambda e, j=j: rows_in.at[e, j],),
            (row_sems.at[0, j],),
            (row_sems.at[1, j],),
        )
        for j in range(local_experts)
    ]
    for copy in row_copies[0] + row_copies[1]:
        copy.start()

    normed = normalize(mix_ref[...], mix_gain_ref[...]).astype(BF16)
    rows = normed.shape[0]
    half = rows // 2
    pair_sums = iota((LANES, LANES), 0) // HEAD == iota((LANES, LANES), 1) // HEAD
    turned = head_turner(
        (ep_me * tp_count + tp_me) * rows, rows, powers_ref[...], pair_sums.astype(BF16)
    )
    query_gain = jnp.concatenate([query_gain_ref[...]] * (LANES // HEAD), axis=1)
    key_gain = jnp.concatenate([key_gain_ref[...]] * (LANES // HEAD), axis=1)
    lower = iota((rows, LANES), 1) < HEAD
    lower_half = iota((half, LANES), 1) < HEAD
    for load in loads[:3]:
        load.wait()
    raw_keys, raw_values = matmul(normed, w_key[...]), matmul(normed, w_value[...])
    key_heads = w_key.shape[1] // HEAD
    group = tp_count // key_heads
    for t in range(key_heads // 2):
        key = turned(raw_keys[:, t * LANES : (t + 1) * LANES], key_gain)
        value = raw_values[:, t * LANES : (t + 1) * LANES].astype(BF16).astype(F32)
        for h, pairs in enumerate(
            (
                jnp.where(lower, key, pltpu.roll(value, HEAD, 1)),
                jnp.where(lower, pltpu.roll(key, HEAD, 1), value),
            )
        ):
            pairs = pairs.astype(BF16)
            for member in range(group):
                part = member % 2 * half
                head_send[(2 * t + h) * group + member, :half, :] = pairs[part : part + half]
    raw_queries = matmul(normed, w_query[...])
    for t in range(tp_count // 2):
        tile = turned(raw_queries[:, t * LANES : (t + 1) * LANES], query_gain)
        first, second = tile[:half], tile[half:]
        head_send[2 * t, half:, :] = jnp.where(
            lower_half, first, pltpu.roll(second, HEAD, 1)
        ).astype(BF16)
        head_send[2 * t + 1, half:, :] = jnp.where(
            lower_half, pltpu.roll(first, HEAD, 1), second
        ).astype(BF16)
    head_copies = exchange_copies(
        "tp",
        (lambda t: head_send.at[t],),
        (lambda t: head_recv.at[t],),
        (head_sems.at[0],),
        (head_sems.at[1],),
    )
    for copy in head_copies:
        copy.start()
    head_recv[tp_me] = head_send[tp_me]
    rows_in[ep_me] = rows_send[ep_me]
    row_max[...] = jnp.full(row_max.shape, -1e30, F32)
    row_sum[...] = jnp.zeros(row_sum.shape, F32)
    row_acc[...] = jnp.zeros(row_acc.shape, F32)

    pieces, _, piece_rows, _ = held.shape
    held_main = ep_count * main_cap

    def receive_rows(j):
        for copy in row_copies[j]:
            copy.wait_recv()
        tiles = rows_in[:, j, column_tiles].reshape(ep_count * column_tiles, LANES)
        for c in range(column_tiles):
            columns = slice(c * LANES, (c + 1) * LANES)
            chosen = matmul(pick(ep_count, ep_count * column_tiles, c, column_tiles), tiles)
            held[j, 0, :held_main, columns] = rows_in[:, j, c].reshape(held_main, LANES)
            held[j, 0, held_main:, columns] = chosen.astype(BF16)

    def ring_copy(i):
        return remote(
            held.at[i, 0], held.at[i + 2, 0], ring_sems.at[0, i], ring_sems.at[1, i], ahead
        )

    def pair_copy(i):
        return remote(
            held.at[i, 0], held.at[i, 1], pair_sems.at[0, i], pair_sems.at[1, i], partner
        )

    def part_copy(i):
        return remote(
            pair_part.at[i], pair_in.at[i], part_sems.at[0, i], part_sems.at[1, i], partner
        )

    def sum_copy(m):
        return remote(leaving.at[m], arrived.at[m], sum_sems.at[0, m], sum_sems.at[1, m], ahead)

    own_keys = head_recv.at[:, pl.ds(0, half), :]
    key_copies = [
        remote(
            own_keys, keys.at[core, d], key_sems.at[0, d], key_sems.at[1, d], {"ep": peer}
        )
        for d, peer in enumerate(axis_peers("ep"))
        if d > 0
    ]

    def key_arrival(d):
        return remote(
            keys.at[core, d], keys.at[core, d], key_sems.at[0, d], key_sems.at[1, d], partner
        )

    def share(d):
        return remote(
            keys.at[core, d], keys.at[core, d], share_sems.at[0, d], share_sems.at[1, d], partner
        )

    tiles_count, tile_rows, _ = row_acc.shape
    tile_groups = tile_rows // rows
    groups = tp_count
    key_group = ep_count // KEY_GROUPS
    key_rows = key_group * groups * half

    def attend_slice(tile, block):
        chosen = queries[tile * tile_groups : (tile + 1) * tile_groups].reshape(tile_rows, LANES)
        pairs = keys[lax.rem(block, 2), pl.ds(block // 2 * key_group, key_group)]
        pairs = pairs.reshape(key_rows, LANES)
        scores = lax.dot_general(
            chosen, pairs, (((1,), (1,)), ((), ())), preferred_element_type=F32
        )
        old_max = row_max[tile][:, :1]
        new_max = jnp.maximum(old_max, jnp.max(scores, axis=1, keepdims=True))
        shrink = jnp.exp2((old_max - new_max) * EXP2_SCALE)
        raised = jnp.exp2((scores - new_max) * EXP2_SCALE)
        lane_sums = raised[:, :LANES]
        for lane in range(LANES, key_rows, LANES):
            lane_sums = lane_sums + raised[:, lane : lane + LANES]
        row_max[tile] = jnp.broadcast_to(new_max, (tile_rows, LANES))
        row_sum[tile] = row_sum[tile] * shrink + lane_sums
        row_acc[tile] = row_acc[tile] * shrink + matmul(raised.astype(BF16), pairs)

    back_copies = [
        exchange_copies(
            "ep",
            (lambda e, j=j: rows_back.at[e, j],),
            (lambda e, j=j: rows_recv.at[e, j],),
            (back_sems.at[0, j],),
            (back_sems.at[1, j],),
        )
        for j in range(local_experts)
    ]
    mixed_copies = exchange_copies(
        "tp",
        (lambda t: mixed_send.at[t],),
        (lambda t: mixed_recv.at[t],),
        (mixed_sems.at[0],),
        (mixed_sems.at[1],),
    )

    def return_rows(j, total):
        tiles = jnp.zeros((ep_count * column_tiles, LANES), F32)
        for c in range(column_tiles):
            columns = slice(c * LANES, (c + 1) * LANES)
            rows_back[:, j, c] = total[:held_main, columns].reshape(ep_count, main_cap, LANES)
            spot = place(ep_count * column_tiles, ep_count, c, column_tiles)
            tiles = tiles + matmul(spot, total[held_main:, columns])
        tiles = tiles.astype(BF16).reshape(ep_count, main_cap, LANES)
        rows_back[:, j, column_tiles] = tiles
        for copy in back_copies[j]:
            copy.start()

    def step(i, _):
        @pl.when(jnp.logical_and(i >= 2, i < pieces + 2))
        def _():
            part_copy(i - 2).start()

        for j in range(local_experts):

            @pl.when(i == j)
            def _(j=j):
                receive_rows(j)

        @pl.when(i < pieces)
        def _():
            @pl.when(i >= 2)
            def _():
                ring_copy(i - 2).wait_recv()

            @pl.when(i < pieces - 2)
            def _():
                ring_copy(i).start()

            pair_copy(i).start()

        @pl.when(i == 1)
        def _():
            for load in loads[3:]:
                load.wait()

        @pl.when(i == 2)
        def _():
            for copy in head_copies:
                copy.wait_recv()
            for copy in key_copies:
                copy.start()
            keys[core, 0] = head_recv[:, :half, :]
            packed = head_recv[:, half:, :].astype(F32).reshape(groups * half, LANES)
            lower_lanes = iota(packed.shape, 1) < HEAD
            for h, values in enumerate((packed, pltpu.roll(packed, HEAD, 1))):
                values = jnp.where(lower_lanes, values, 0.0).astype(BF16)
                queries[:, h * half : (h + 1) * half, :] = values.reshape(groups, half, LANES)

        @pl.when((i >= 5) & (i < 5 + 2 * KEY_GROUPS) & (lax.rem(i, 2) == 1))
        def _():
            for g in range(key_group):
                d = (i - 5) // 2 * key_group + g

                @pl.when(d > 0)
                def _():
                    key_arrival(d).wait_recv()

                share(d).start()

        @pl.when(jnp.logical_and(i >= 1, i <= pieces))
        def _():
            piece = i - 1
            expert = lax.rem(piece, 2)
            pair_copy(piece).wait_recv()
            values = held[piece].reshape(2 * piece_rows, width)
            gate_act = matmul(values, gate[expert])
            up_act = matmul(values, up[expert])
            hidden = (gate_act / (1.0 + jnp.exp(-gate_act)) * up_act).astype(BF16)
            sums = matmul(hidden, down[expert]).astype(BF16)
            own_part[piece] = sums[:piece_rows]
            pair_part[piece] = sums[piece_rows:]

        @pl.when(jnp.logical_and(i >= 7, i < 7 + 2 * KEY_GROUPS))
        def _():
            block = i - 7

            @pl.when(lax.rem(block, 2) == 0)
            def _():
                for g in range(key_group):
                    share(block // 2 * key_group + g).wait_recv()

            for tile in range(tiles_count):
                attend_slice(tile, block)

        @pl.when(i >= 4)
        def _():
            m = i - 4
            piece = lax.rem(m + 2, pieces)
            part_copy(piece).wait_recv()

            @pl.when(m < 2)
            def _():
                total = own_part[piece].astype(F32) + pair_in[piece].astype(F32)
                leaving[m] = total.astype(BF16)

            @pl.when(m >= 2)
            def _():
                sum_copy(m - 2).wait_recv()
                total = own_part[piece].astype(F32) + pair_in[piece].astype(F32)
                total = (total + arrived[m - 2].astype(F32)).astype(BF16)

                @pl.when(m < pieces - 2)
                def _():
                    leaving[m] = total

                for j in range(local_experts):

                    @pl.when(m == pieces - 2 + j)
                    def _(j=j):
                        return_rows(j, total)

            @pl.when(m < pieces - 2)
            def _():
                sum_copy(m).start()

        @pl.when(i == pieces)
        def _():
            for tile in range(tiles_count):
                mixed = row_acc[tile] / jnp.sum(row_sum[tile], axis=1, keepdims=True)
                mixed = mixed.reshape(tile_groups, rows, LANES)
                first = mixed[:, :half].reshape(tile_groups * half, LANES)
                second = mixed[:, half:].reshape(tile_groups * half, LANES)
                upper = iota(first.shape, 1) >= HEAD
                mixed = jnp.where(upper, second, pltpu.roll(first, HEAD, 1)).astype(BF16)
                mixed_send[tile * tile_groups : (tile + 1) * tile_groups] = mixed.reshape(
                    tile_groups, half, LANES
                )

        return 0

    lax.fori_loop(0, pieces + 4, step, 0)
    for copy in mixed_copies:
        copy.start()
    mixed_recv[tp_me] = mixed_send[tp_me]
    rows_recv[ep_me] = rows_back[ep_me]
    for copy in row_copies[0] + row_copies[1] + head_copies:
        copy.wait_send()

    def finish(i, _):
        @pl.when(i < pieces - 2)
        def _():
            ring_copy(i).wait_send()
            sum_copy(i).wait_send()

        pair_copy(i).wait_send()
        part_copy(i).wait_send()
        return 0

    lax.fori_loop(0, pieces, finish, 0)
    for copy in key_copies:
        copy.wait_send()

    def finish_share(d, _):
        share(d).wait_send()
        return 0

    lax.fori_loop(0, ep_count, finish_share, 0)

    main, last = slot_rows(ids_ref[...], experts, capacity)
    takers = []
    for k in range(len(main)):
        slot = jnp.where(main[k] >= 0, main[k], jnp.where(last[k] >= 0, last[k] + main_rows, -1))
        spot = (iota((results.shape[0], tokens), 0) == slot).astype(F32)
        takers.append(jnp.transpose(spot).astype(BF16))
    results[main_rows:, :] = jnp.zeros((results.shape[0] - main_rows, width), BF16)
    for copy in mixed_copies:
        copy.wait()
    heads = []
    for t in range(tp_count // 2):
        even, odd = mixed_recv[2 * t].astype(F32), mixed_recv[2 * t + 1].astype(F32)
        first = jnp.where(lower_half, even, pltpu.roll(odd, HEAD, 1))
        second = jnp.where(lower_half, pltpu.roll(even, HEAD, 1), odd)
        heads.append(jnp.concatenate([first, second], axis=0).astype(BF16))
    mix_out[...] = matmul(jnp.concatenate(heads, axis=1), w_out[...]).astype(BF16)

    for copy in back_copies[0] + back_copies[1]:
        copy.wait()
    tiles = rows_recv[:, :, column_tiles].reshape(last_rows, LANES)
    for c in range(column_tiles):
        columns = slice(c * LANES, (c + 1) * LANES)
        results[:main_rows, columns] = rows_recv[:, :, c].reshape(main_rows, LANES)
        chosen = matmul(pick(experts, last_rows, c, column_tiles), tiles)
        results[main_rows : main_rows + experts, columns] = chosen.astype(BF16)
    combined = jnp.zeros((tokens, width), F32)
    for k, taker in enumerate(takers):
        row = jnp.broadcast_to(weights_ref[k : k + 1, :], (tokens, tokens))
        combined = combined + jnp.transpose(row)[:, :1] * matmul(taker, results[...])
    experts_out[...] = combined.astype(BF16)


def layer(
    mix, mix_gain, w_query, w_key, w_value, query_gain, key_gain, powers, w_out, tokens, gain, ids,
    weights, w_gate, w_up, w_down, capacity,
):
    pieces, ep_count = lax.axis_size("tp"), lax.axis_size("ep")
    rows, width = mix.shape
    local_experts = w_gate.shape[0]
    piece = (ep_count * capacity, width)
    head = pltpu.VMEM((pieces, rows, LANES), BF16)
    packed = pltpu.VMEM((pieces, rows // 2, LANES), BF16)
    query_tile = math.gcd(pieces * rows, 256)
    state = pltpu.VMEM((pieces * rows // query_tile, query_tile, LANES), F32)
    column_tiles = width // LANES
    assert column_tiles == capacity - 1
    block = pltpu.VMEM((ep_count, local_experts, column_tiles + 1, capacity - 1, LANES), BF16)
    sums = pltpu.VMEM((pieces,) + piece, BF16)
    flights = pltpu.VMEM((pieces - 2,) + piece, BF16)
    result_rows = -(-local_experts * ep_count * capacity // LANES) * LANES
    return pl.pallas_call(
        layer_body,
        out_shape=[
            jax.ShapeDtypeStruct((rows, w_out.shape[1]), BF16),
            jax.ShapeDtypeStruct(tokens.shape, BF16),
        ],
        in_specs=[VMEM_SPEC] * 2
        + [HBM_SPEC] * 3
        + [VMEM_SPEC] * 3
        + [HBM_SPEC]
        + [VMEM_SPEC] * 4
        + [HBM_SPEC] * 3,
        out_specs=[VMEM_SPEC] * 2,
        scratch_shapes=[
            pltpu.VMEM(w.shape, BF16) for w in (w_query, w_key, w_value, w_out, w_gate, w_up, w_down)
        ]
        + [head, head, block, block]
        + [pltpu.VMEM((pieces, 2) + piece, BF16), sums, sums, sums, flights, flights]
        + [pltpu.VMEM((2, ep_count, pieces, rows // 2, LANES), BF16), head, state, state, state]
        + [packed, packed, block, block]
        + [pltpu.VMEM((result_rows, width), BF16)]
        + [DMA((7,)), DMA((2, pieces)), DMA((2, local_experts, ep_count))]
        + [DMA((2, pieces))] * 4
        + [DMA((2, ep_count))] * 2
        + [DMA((2, pieces)), DMA((2, local_experts, ep_count))],
        name="layer",
        compiler_params=pltpu.CompilerParams(
            collective_id=0, has_side_effects=True, vmem_limit_bytes=62 * MIB
        ),
    )(
        mix, mix_gain, w_query, w_key, w_value, query_gain, key_gain, powers, w_out, tokens, gain,
        ids, weights, w_gate, w_up, w_down,
    )


def body(
    mix_tokens,
    mix_gain,
    w_query,
    w_key,
    w_value,
    query_gain,
    key_gain,
    w_out,
    expert_tokens,
    expert_gain,
    route_ids,
    route_weights,
    w_gate,
    w_up,
    w_down,
):
    ep_count = lax.axis_size("ep")
    seq_rows, _, model_width = mix_tokens.shape
    tok_count, top_count = route_ids.shape
    local_experts = w_gate.shape[0]
    capacity = tok_count * top_count * 9 // (8 * local_experts * ep_count)
    id_rows = jnp.transpose(route_ids)
    mix_out, experts_out = layer(
        mix_tokens.reshape(seq_rows, model_width),
        mix_gain.reshape(1, model_width),
        w_query,
        w_key,
        w_value,
        query_gain.reshape(1, HEAD),
        key_gain.reshape(1, HEAD),
        frequencies(),
        w_out,
        expert_tokens,
        expert_gain.reshape(1, model_width),
        id_rows,
        jnp.transpose(route_weights),
        w_gate,
        w_up,
        w_down,
        capacity,
    )
    return (mix_out[:, None, :], experts_out)


def solution(mesh):
    placed = (
        P(("ep", "tp"), None, None),
        P(),
        P(),
        P(),
        P(),
        P(),
        P(),
        P(),
        P(("ep", "tp"), None),
        P(),
        P(("ep", "tp"), None),
        P(("ep", "tp"), None),
        P("ep", None, "tp"),
        P("ep", None, "tp"),
        P("ep", "tp", None),
    )
    return jax.shard_map(
        body,
        mesh=mesh,
        in_specs=placed,
        out_specs=(P(("ep", "tp"), None, None), P(("ep", "tp"), None)),
        check_vma=False,
    )
```
